32 devices in a mesh: ep: 8 (over z, y), tp: 4 (over x, core).
Axes of the slice: x: 2, y: 2, z: 4, core: 2. Of those that a mesh axis runs over, the one named last changes fastest.
Arguments:
- queries: bfloat16 [1536, 2048], P('ep', 'tp'), may hold values from -5 to 5
- keys: bfloat16 [1536, 512], P('ep', 'tp'), may hold values from -5 to 5
- values: bfloat16 [1536, 512], P('ep', 'tp'), may hold values from -6 to 6
- query_gain: float32 [128], replicated, may hold values from 0.6 to 6
- key_gain: float32 [128], replicated, may hold values from 0.6 to 6
- out_weight: bfloat16 [2048, 2048], P('tp'), may hold values from -0.125 to 0.125
- mixer_gain: float32 [2048], replicated, may hold values from 0.1 to 1.9
- expert_in: bfloat16 [4096, 2048], P(('ep', 'tp')), may hold values from -6 to 6
- routes: int32 [4096, 2], P(('ep', 'tp')), may hold values from 0 to 7, all different within a row; in each aligned block of 128 rows (0 to 127, 128 to 255, ...) at most 48 rows name the same one
- route_weights: float32 [4096, 2], P(('ep', 'tp')), may hold values from 0.2 to 1
- expert_gain: float32 [2048], replicated, may hold values from 0.5 to 4
- gate_w: bfloat16 [8, 2048, 2048], P('ep', None, 'tp'), may hold values from -0.125 to 0.125
- up_w: bfloat16 [8, 2048, 2048], P('ep', None, 'tp'), may hold values from -0.125 to 0.125
- down_w: bfloat16 [8, 2048, 2048], P('ep', 'tp'), may hold values from -0.125 to 0.125
- ffn_out_gain: float32 [2048], replicated, may hold values from 0.1 to 1.9
Outputs:
- mixer_out: bfloat16 [1536, 2048], P(('ep', 'tp'))
- expert_out: bfloat16 [4096, 2048], P(('ep', 'tp'))
The draws below stay inside these ranges and needn't reach their ends.
Inputs may be any that keep to these rules, and one draw needn't show every extreme that they name: `routes`: each row names 2 different experts. Among the rows of one device no expert is named by more than 48 rows, and in every draw some expert is named by exactly 48 rows of some device.
All inputs are finite; a program needn't handle non-finite values.
Results may differ from the reference program's by a relative error of at most 0.015.
The reference program's roundings to bfloat16 on the way count: a program that leaves them out, or rounds other values in their place, can miss the bound.
Values may be sent and summed in bfloat16 or wider, within the bound.
A program may use at most 128 MiB of HBM per device.

```python
import math
import jax
import jax.numpy as jnp
import numpy as np
from jax import lax

D = 2048
HEADS = 16
KV_HEADS = 4
HEAD = 128
QW = 2048
KVW = 512
GRID_W = 64
LEN = 1536
FF = 2048
TOPK = 2
TB_DEV = 128
EXPERTS = 8
CAP = 48
TOKB = 4096
N_EP = 8
N_TP = 4


def plant_pairs(key):
    base_key = jax.random.fold_in(key, 7)
    key_part = jnp.clip(jax.random.normal(jax.random.fold_in(base_key, 1), (LEN, KVW), jnp.float32), -5.0, 5.0)
    query_part = jnp.clip(jax.random.normal(jax.random.fold_in(base_key, 2), (LEN, QW), jnp.float32), -5.0, 5.0)
    return (query_part, key_part)


def draw_queries(key, part):
    return plant_pairs(key)[0].astype(jnp.bfloat16)


def draw_keys(key, part):
    return plant_pairs(key)[1].astype(jnp.bfloat16)


def pair_gain(key, salt):
    base_key = jax.random.fold_in(key, salt)
    return jax.random.uniform(base_key, (HEAD,), jnp.float32, 0.6, 1.4)


def draw_query_gain(key, part):
    return pair_gain(key, 11)


def draw_key_gain(key, part):
    return pair_gain(key, 12)


def steps_of(key, shape, shards, least, top_value):
    def one(dim, blocks):
        heights = jax.random.uniform(jax.random.fold_in(jax.random.fold_in(key, 6), dim), (blocks,), jnp.float32, least / len(shards), top_value / len(shards))
        return jnp.repeat(jnp.exp(heights), shape[dim] // blocks).reshape((-1,) + (1,) * (len(shape) - dim - 1))

    level = one(*shards[0])
    for cut in shards[1:]:
        level = level * one(*cut)
    return level


def routed_block(stream_key, own, number, rows, number_of, top, most, slope):
    order = jax.random.permutation(stream_key, number_of)
    heavy_load, ordinary = shares(number_of, rows * top, most, slope, True), shares(number_of, rows * top, most, slope, False)
    places = jnp.arange(number_of)

    def named(tallies, turn):
        used = int((tallies > 0).sum())
        fixed = max(1, used // 4)
        shifted = fixed + (places - fixed + turn * (used - fixed)) % max(1, number_of - fixed)
        return jnp.zeros((number_of,), jnp.int32).at[order[jnp.where(places < fixed, places, shifted)]].set(jnp.asarray(tallies, jnp.int32))

    tallies = jnp.where(number % 4 == 0, named(heavy_load, number // 4), named(ordinary, number - number // 4 - 1))
    mixed = jax.random.permutation(jax.random.fold_in(own, 3), number_of)
    source_of, receiver = mixed[0:number_of // 2 * 2:2], mixed[1:number_of // 2 * 2:2]
    slack = jnp.minimum(tallies[source_of] - 1, most - tallies[receiver]) // 2
    slack = jnp.where((source_of == order[0]) | (receiver == order[0]) | (tallies[receiver] == 0), 0, jnp.maximum(slack, 0))
    shifted = jax.random.randint(jax.random.fold_in(own, 4), (number_of // 2,), 0, 1 << 20) % (slack + 1)
    tallies = tallies.at[source_of].add(-shifted).at[receiver].add(shifted)
    labels = jnp.searchsorted(jnp.cumsum(tallies), jnp.arange(rows * top), side="right").astype(jnp.int32)
    table = labels.reshape(top, rows).T
    table = table[jax.random.permutation(jax.random.fold_in(own, 1), rows)]
    turn = jax.random.randint(jax.random.fold_in(own, 2), (rows, 1), 0, top)
    return jnp.take_along_axis(table, (jnp.arange(top)[None, :] + turn) % top, axis=1)


def shares(number_of, total, most, lean, full):
    loads = [(1 << 20) // math.isqrt(standing ** lean) + 1 for standing in range(1, number_of + 1)]
    largest = most if full else min(most, max(-(-total // number_of), total * loads[0] // sum(loads)))
    least = 1 if total - largest >= number_of - 1 else 0
    given, spare = [largest] + [least] * (number_of - 1), total - largest - least * (number_of - 1)
    while spare > 0:
        movable = [i for i in range(1, number_of) if given[i] < largest] or [i for i in range(1, number_of) if given[i] < most]
        mass, left = sum([loads[i] for i in movable]), spare
        for i in movable:
            more = min(most - given[i], max(1, left * loads[i] // mass), spare)
            given[i] = given[i] + more
            spare = spare - more
    return np.array(given)


def scatter_about(key, shape, scale, reach, cuts=(), kind=jnp.bfloat16):
    entries = scale * jax.random.normal(key, shape, jnp.float32)
    if cuts:
        entries = entries * steps_of(key, shape, cuts, -0.22, 0.18)
    return jnp.clip(entries, -reach, reach).astype(kind)


def setup_inputs(seed: int = 0) -> dict:
    seeds = jax.random.split(jax.random.key(seed), 16)
    queries = draw_queries(jax.random.fold_in(seeds[15], 71), 0)
    keys = draw_keys(jax.random.fold_in(seeds[15], 71), 0)
    values = scatter_about(seeds[2], (LEN, KVW), 1.0, 6.0, ((0, 8), (1, 4)))
    query_gain = draw_query_gain(jax.random.fold_in(seeds[15], 71), 0)
    key_gain = draw_key_gain(jax.random.fold_in(seeds[15], 71), 0)
    out_weight = scatter_about(seeds[5], (QW, D), QW ** -0.5, 0.125, ((0, 4),))
    mixer_gain = jnp.clip(1.0 + 0.18 * jax.random.normal(seeds[6], (D,), jnp.float32), 0.1, 1.9)
    expert_in = scatter_about(seeds[7], (TOKB, D), 1.0, 6.0, ((0, 32),))
    routes_keys = jax.random.split(jax.random.fold_in(seeds[8], 1), TOKB // TB_DEV)
    routes_turns = jax.random.permutation(jax.random.fold_in(seeds[8], 3), TOKB // TB_DEV)
    routes = jax.vmap(lambda own, number: routed_block(jax.random.fold_in(seeds[8], 2), own, number, TB_DEV, EXPERTS, TOPK, CAP, 1))(routes_keys, routes_turns).reshape((TOKB, TOPK))
    route_weights = jnp.clip(0.2 + 0.8 * jax.random.uniform(seeds[9], (TOKB, TOPK), jnp.float32) ** steps_of(seeds[9], (TOKB, TOPK), ((0, 32),), -0.2, 0.2), 0.2, 1.0)
    expert_gain = jnp.clip(jnp.exp(jax.random.uniform(seeds[10], (D,), jnp.float32, math.log(0.5), math.log(4.0))), 0.5, 4.0)
    gate_w = scatter_about(seeds[11], (EXPERTS, D, FF), D ** -0.5, 0.125, ((0, 8), (2, 4)))
    up_w = scatter_about(seeds[12], (EXPERTS, D, FF), D ** -0.5, 0.125, ((0, 8), (2, 4)))
    down_w = scatter_about(seeds[13], (EXPERTS, FF, D), FF ** -0.5, 0.125, ((0, 8), (1, 4)))
    ffn_out_gain = jnp.clip(1.0 + 0.18 * jax.random.normal(seeds[14], (D,), jnp.float32), 0.1, 1.9)
    return {"queries": queries, "keys": keys, "values": values, "query_gain": query_gain, "key_gain": key_gain, "out_weight": out_weight, "mixer_gain": mixer_gain, "expert_in": expert_in, "routes": routes, "route_weights": route_weights, "expert_gain": expert_gain, "gate_w": gate_w, "up_w": up_w, "down_w": down_w, "ffn_out_gain": ffn_out_gain}


norm_eps = 1e-06
rope_base = 10000.0
clamp_limit = 7.0
sigmoid_slope = 1.702

def rms_scale(values_in, gain):
    return values_in * lax.rsqrt(lax.optimization_barrier(jnp.mean(values_in * values_in, axis=-1, keepdims=True)) + norm_eps) * gain

def turn_pair(halfpart, cosine, sine):
    first_part, second_part = jnp.split(halfpart, 2, axis=-1)
    return jnp.concatenate([first_part * cosine - second_part * sine, second_part * cosine + first_part * sine], axis=-1)

def grid_rotate(field, position):
    half_width = field.shape[-1] // 2
    inverse = rope_base ** (-jnp.arange(0, half_width, 2, dtype=jnp.float32) / half_width)
    grid_row = (position // GRID_W).astype(jnp.float32)
    grid_col = (position % GRID_W).astype(jnp.float32)
    row_angle = (grid_row[:, None] * inverse[None, :])[:, None, :]
    col_angle = (grid_col[:, None] * inverse[None, :])[:, None, :]
    return jnp.concatenate([turn_pair(field[..., :half_width], jnp.cos(row_angle), jnp.sin(row_angle)), turn_pair(field[..., half_width:], jnp.cos(col_angle), jnp.sin(col_angle))], axis=-1)

def clamped_unit(gate_pre, up_pre):
    gate_cut = jnp.minimum(gate_pre, clamp_limit)
    up_cut = jnp.clip(up_pre, -clamp_limit, clamp_limit)
    return ((up_cut + 1.0) * gate_cut * jax.nn.sigmoid(sigmoid_slope * gate_cut)).astype(jnp.bfloat16)

def reference(queries, keys, values, query_gain, key_gain, out_weight, mixer_gain, expert_in, routes, route_weights, expert_gain, gate_w, up_w, down_w, ffn_out_gain):
    group_size = HEADS // KV_HEADS
    position = jnp.arange(LEN, dtype=jnp.int32)
    query_norm = grid_rotate(rms_scale(queries.astype(jnp.float32).reshape(LEN, HEADS, HEAD), query_gain), position).astype(jnp.bfloat16)
    key_norm = grid_rotate(rms_scale(keys.astype(jnp.float32).reshape(LEN, KV_HEADS, HEAD), key_gain), position).astype(jnp.bfloat16)
    key_wide = key_norm.astype(jnp.float32)
    value_wide = values.reshape(LEN, KV_HEADS, HEAD).astype(jnp.float32)
    score_scale = HEAD ** (-0.5)
    query_blocks = query_norm.reshape(LEN // GRID_W, GRID_W, KV_HEADS, group_size, HEAD)

    def attend_block(block_in):
        scores = jnp.einsum('qhgd,khd->hgqk', block_in.astype(jnp.float32), key_wide) * score_scale
        expo = jnp.exp(scores - lax.optimization_barrier(jnp.max(scores, axis=-1, keepdims=True)))
        total = lax.optimization_barrier(jnp.sum(expo, axis=-1))
        probs = lax.optimization_barrier(expo.astype(jnp.bfloat16))
        summed = jnp.einsum('hgqk,khd->qhgd', probs.astype(jnp.float32), value_wide)
        return (summed / jnp.transpose(total, (2, 0, 1))[..., None]).astype(jnp.bfloat16)
    attended = lax.map(attend_block, query_blocks).reshape(LEN, HEADS * HEAD)
    column_span = HEADS * HEAD // N_TP
    projected = jnp.zeros((LEN, D), jnp.float32)
    for member in range(N_TP):
        partial_term = jnp.dot(attended[:, member * column_span:(member + 1) * column_span], out_weight[member * column_span:(member + 1) * column_span], preferred_element_type=jnp.float32).astype(jnp.bfloat16)
        projected = projected + lax.optimization_barrier(partial_term).astype(jnp.float32)
    mixer_out = rms_scale(projected, mixer_gain).astype(jnp.bfloat16)
    normed = rms_scale(expert_in.astype(jnp.float32), expert_gain).astype(jnp.bfloat16)
    padded = jnp.concatenate([normed, jnp.zeros((1, D), jnp.bfloat16)], axis=0)
    pair_expert = routes.reshape(-1)
    pair_count = pair_expert.shape[0]
    pair_weight = jnp.concatenate([route_weights.reshape(-1), jnp.zeros((1,), jnp.float32)], axis=0)
    most_rows = N_EP * N_TP * CAP
    hidden_span = FF // N_TP

    def one_expert(combined_in, expert_id):
        chosen = jnp.nonzero(pair_expert == expert_id, size=most_rows, fill_value=pair_count)[0].astype(jnp.int32)
        token_index = chosen // TOPK
        inputs = padded[token_index]
        hidden = clamped_unit(jnp.dot(inputs, gate_w[expert_id], preferred_element_type=jnp.float32), jnp.dot(inputs, up_w[expert_id], preferred_element_type=jnp.float32))
        down_here = down_w[expert_id]
        result = jnp.zeros((most_rows, D), jnp.float32)
        for member in range(N_TP):
            partial_term = jnp.dot(hidden[:, member * hidden_span:(member + 1) * hidden_span], down_here[member * hidden_span:(member + 1) * hidden_span], preferred_element_type=jnp.float32).astype(jnp.bfloat16)
            result = result + lax.optimization_barrier(partial_term).astype(jnp.float32)
        output_rows = lax.optimization_barrier(result.astype(jnp.bfloat16))
        combined_out = combined_in.at[token_index].add(pair_weight[chosen][:, None] * output_rows.astype(jnp.float32))
        return (combined_out, None)
    combined, unused = lax.scan(one_expert, jnp.zeros((TOKB + 1, D), jnp.float32), jnp.arange(EXPERTS, dtype=jnp.int32))
    expert_out = rms_scale(combined[:TOKB], ffn_out_gain).astype(jnp.bfloat16)
    return (mixer_out, expert_out)
```

```python
import jax
import jax.numpy as jnp
import numpy as np
from jax import lax
from jax.experimental import pallas as pl
from jax.experimental.pallas import tpu as pltpu
from jax.sharding import PartitionSpec as P

HEAD = 128
GRID_W = 64


norm_eps = 1e-06
rope_base = 10000.0
clamp_limit = 7.0
sigmoid_slope = 1.702


def rms_scale(values_in, gain):
    return (
        values_in
        * lax.rsqrt(jnp.mean(values_in * values_in, axis=-1, keepdims=True) + norm_eps)
        * gain
    )


def turn_pair(halfpart, cosine, sine):
    first_part, second_part = jnp.split(halfpart, 2, axis=-1)
    return jnp.concatenate(
        [first_part * cosine - second_part * sine, second_part * cosine + first_part * sine],
        axis=-1,
    )


def grid_rotate(field, position):
    half_width = field.shape[-1] // 2
    inverse = rope_base ** (-jnp.arange(0, half_width, 2, dtype=jnp.float32) / half_width)
    grid_row = (position // GRID_W).astype(jnp.float32)
    grid_col = (position % GRID_W).astype(jnp.float32)
    row_angle = (grid_row[:, None] * inverse[None, :])[:, None, :]
    col_angle = (grid_col[:, None] * inverse[None, :])[:, None, :]
    return jnp.concatenate(
        [
            turn_pair(field[..., :half_width], jnp.cos(row_angle), jnp.sin(row_angle)),
            turn_pair(field[..., half_width:], jnp.cos(col_angle), jnp.sin(col_angle)),
        ],
        axis=-1,
    )


def clamped_unit(gate_pre, up_pre):
    gate_cut = jnp.minimum(gate_pre, clamp_limit)
    up_cut = jnp.clip(up_pre, -clamp_limit, clamp_limit)
    return ((up_cut + 1.0) * gate_cut * jax.nn.sigmoid(sigmoid_slope * gate_cut)).astype(
        jnp.bfloat16
    )


def mixer_half(queries, keys, values, query_gain, key_gain, out_weight, mixer_gain):
    local_rows = queries.shape[0]
    kv_local = keys.shape[1] // HEAD
    group_size = queries.shape[1] // HEAD // kv_local
    position = lax.axis_index("ep") * local_rows + jnp.arange(local_rows, dtype=jnp.int32)
    query_f = queries.astype(jnp.float32).reshape(local_rows, kv_local * group_size, HEAD)
    query_norm = grid_rotate(rms_scale(query_f, query_gain), position).astype(jnp.bfloat16)
    query_norm = query_norm.reshape(local_rows, kv_local, group_size, HEAD)
    key_f = keys.astype(jnp.float32).reshape(local_rows, kv_local, HEAD)
    key_norm = grid_rotate(rms_scale(key_f, key_gain), position).astype(jnp.bfloat16)
    key_norm = key_norm.reshape(local_rows, kv_local * HEAD)
    score_scale = HEAD ** (-0.5)
    initial = (
        jnp.full((kv_local, group_size, local_rows), -1e30, jnp.float32),
        jnp.zeros((kv_local, group_size, local_rows), jnp.float32),
        jnp.zeros((kv_local, group_size, local_rows, HEAD), jnp.float32),
    )
    key_piece = lax.all_gather(key_norm, "ep", axis=0, tiled=True)
    value_piece = lax.all_gather(values, "ep", axis=0, tiled=True)
    piece_rows = key_piece.shape[0]
    block_rows = 1
    for candidate in range(min(piece_rows, 1024), 0, -1):
        if piece_rows % candidate == 0:
            block_rows = candidate
            break
    key_blocks = key_piece.reshape(piece_rows // block_rows, block_rows, kv_local, HEAD)
    value_blocks = value_piece.reshape(piece_rows // block_rows, block_rows, kv_local, HEAD)

    def one_block(state, blocks_in):
        running_max, running_total, weighted = state
        key_block, value_block = blocks_in
        scores = (
            jnp.einsum("qhgd,khd->hgqk", query_norm, key_block, preferred_element_type=jnp.float32)
            * score_scale
        )
        new_max = jnp.maximum(running_max, jnp.max(scores, axis=-1))
        factor = jnp.exp(running_max - new_max)
        expo = jnp.exp(scores - new_max[..., None])
        new_total = running_total * factor + jnp.sum(expo, axis=-1)
        new_weighted = weighted * factor[..., None] + jnp.einsum(
            "hgqk,khd->hgqd",
            expo.astype(jnp.bfloat16),
            value_block,
            preferred_element_type=jnp.float32,
        )
        return ((new_max, new_total, new_weighted), None)

    state_out, unused = lax.scan(one_block, initial, (key_blocks, value_blocks))
    final_max, final_total, weighted = state_out
    attended = (weighted / final_total[..., None]).astype(jnp.bfloat16)
    attended = jnp.transpose(attended, (2, 0, 1, 3)).reshape(
        local_rows, kv_local * group_size * HEAD
    )
    share_rows = local_rows // lax.axis_size("tp")
    selected = lax.slice_in_dim(attended, 0, lax.axis_size("tp") * share_rows, axis=0)
    projected = lax.psum_scatter(
        jnp.dot(selected, out_weight, preferred_element_type=jnp.float32).astype(jnp.bfloat16),
        "tp",
        scatter_dimension=0,
        tiled=True,
    ).astype(jnp.float32)
    return rms_scale(projected, mixer_gain).astype(jnp.bfloat16)


def expert_half(expert_in, routes, route_weights, expert_gain, gate_w, up_w, down_w, ffn_out_gain):
    tok_rows = expert_in.shape[0]
    model_width = expert_in.shape[1]
    top_count = routes.shape[1]
    expert_count = lax.axis_size("ep")
    capacity = max(2, (3 * tok_rows * top_count + 2 * expert_count - 1) // (2 * expert_count))
    normed = rms_scale(expert_in.astype(jnp.float32), expert_gain).astype(jnp.bfloat16)
    pair_expert = routes.reshape(-1)
    pair_count = pair_expert.shape[0]
    one_hot = (pair_expert[:, None] == jnp.arange(expert_count, dtype=jnp.int32)[None, :]).astype(
        jnp.int32
    )
    pair_rank = jnp.sum(jnp.cumsum(one_hot, axis=0) * one_hot, axis=1) - 1
    pair_slot = pair_expert * capacity + pair_rank
    slot_pair = (
        jnp.full((expert_count * capacity,), pair_count, jnp.int32)
        .at[pair_slot]
        .set(jnp.arange(pair_count, dtype=jnp.int32))
    )
    padded = jnp.concatenate([normed, jnp.zeros((1, model_width), jnp.bfloat16)], axis=0)
    outgoing = padded[slot_pair // top_count].reshape(expert_count, capacity, model_width)
    gate_local = gate_w[0]
    up_local = up_w[0]
    down_local = down_w[0]
    arrived = lax.all_to_all(outgoing, "ep", split_axis=0, concat_axis=0, tiled=True)
    flat_rows = arrived.reshape(-1, model_width)
    shard_rows = lax.all_gather(flat_rows, "tp", axis=0, tiled=True)
    hidden = clamped_unit(
        jnp.dot(shard_rows, gate_local, preferred_element_type=jnp.float32),
        jnp.dot(shard_rows, up_local, preferred_element_type=jnp.float32),
    )
    selected = lax.slice_in_dim(hidden, 0, lax.axis_size("tp") * flat_rows.shape[0], axis=0)
    result = lax.psum_scatter(
        jnp.dot(selected, down_local, preferred_element_type=jnp.float32).astype(jnp.bfloat16),
        "tp",
        scatter_dimension=0,
        tiled=True,
    )
    finished = result.reshape(arrived.shape)
    returned = lax.all_to_all(finished, "ep", split_axis=0, concat_axis=0, tiled=True)
    pair_result = returned.reshape(-1, model_width)[pair_slot].reshape(
        tok_rows, top_count, model_width
    )
    combined = jnp.einsum("tk,tkd->td", route_weights, pair_result.astype(jnp.float32))
    return rms_scale(combined, ffn_out_gain).astype(jnp.bfloat16)


def flip(index, bits):
    power = 1
    while power <= bits:
        if bits & power:
            index = index + power - 2 * power * lax.rem(lax.div(index, power), 2)
        power *= 2
    return index


def capacity_of(tok_rows, top_count, expert_count):
    return max(2, (3 * tok_rows * top_count + 2 * expert_count - 1) // (2 * expert_count))


def fused_fits(queries, keys, expert_in, routes, gate_w):
    n_ep, n_tp = lax.axis_size("ep"), lax.axis_size("tp")
    rows = queries.shape[0]
    capacity = capacity_of(expert_in.shape[0], routes.shape[1], n_ep)
    width = expert_in.shape[1]
    hidden = gate_w.shape[2]
    slots = n_ep * capacity
    held = 2 * width * slots * 14 + 6 * width * hidden * 4 + 4 * rows * rows * n_ep
    return (
        n_tp == 4
        and n_ep >= 4
        and n_ep & (n_ep - 1) == 0
        and keys.shape[1] == HEAD
        and capacity % 16 == 0
        and rows % (16 * n_tp) == 0
        and rows % GRID_W == 0
        and queries.shape[1] % HEAD == 0
        and expert_in.shape[0] % 16 == 0
        and held < 56 * 2**20
    )


STEPS = (
    "F0", "D2", "W", "D1", "KR", "D3", "K0", "F1", "D4", "F2", "F3", "R2", "R1", "R0", "D6",
    "C2", "F4", "P2", "R3", "K1", "D5", "R4", "F6", "C4", "P4", "C1", "D7", "R6", "G2", "C3",
    "P1", "G4", "K2", "F5", "C6", "P6", "G1", "F7", "R5", "C5", "G6", "P5", "P3", "R7", "C7",
    "G5", "C0", "P7", "A0", "A1", "A2", "G3", "P0", "A3", "O", "M", "G7", "G0", "N", "E",
)


def rope_tables(grid_rows):
    half = HEAD // 2
    lane = np.arange(HEAD)
    inverse = rope_base ** (-2.0 * (lane % (half // 2)) / half)
    sign = np.where(lane % half < half // 2, -1.0, 1.0)
    row = np.arange(grid_rows)[:, None] * inverse[None, :]
    col = np.arange(GRID_W)[:, None] * inverse[None, :]
    low = (lane < half)[None, :]
    tables = (
        np.where(low, np.cos(row), 0.0),
        np.where(low, np.sin(row) * sign, 0.0),
        np.where(low, 0.0, np.cos(col)),
        np.where(low, 0.0, np.sin(col) * sign),
    )
    return [jnp.asarray(t.astype(np.float32)) for t in tables]


def fused_kernel(
    query_hbm,
    key_hbm,
    value_hbm,
    expert_hbm,
    out_w_hbm,
    gate_hbm,
    up_hbm,
    down_hbm,
    query_gain_ref,
    key_gain_ref,
    mixer_gain_ref,
    expert_gain_ref,
    ffn_gain_ref,
    routes_ref,
    route_weight_ref,
    row_cos_ref,
    row_sin_ref,
    col_cos_ref,
    col_sin_ref,
    mixer_out_ref,
    expert_out_ref,
    query,
    key,
    expert_in,
    out_w,
    gate,
    up,
    down,
    kv_all,
    att,
    proj,
    proj_in,
    proj_sum,
    proj_xin,
    outg,
    slot_weight,
    rows,
    part,
    part_in,
    part_sum,
    part_xin,
    final,
    ret,
    load_sem,
    kv_send,
    kv_recv,
    disp_send,
    disp_recv,
    core_send,
    core_recv,
    chip_send,
    chip_recv,
    relay_send,
    relay_recv,
    pcore_send,
    pcore_recv,
    pchip_send,
    pchip_recv,
    ret_send,
    ret_recv,
    mix_send,
    mix_recv,
):
    tok_rows, width = expert_in.shape
    n = disp_send.shape[0]
    cap = ret.shape[0] // n
    local_rows = key.shape[0]
    share = local_rows // 4
    heads = query.shape[1] // HEAD
    grid_rows = local_rows // GRID_W
    bf16, f32 = jnp.bfloat16, jnp.float32
    ep, tp = lax.axis_index("ep"), lax.axis_index("tp")

    def at(ref, start, size):
        return ref.at[pl.ds(start, size), :]

    def remote(src, dst, send, recv, ep_bits, tp_bits):
        return pltpu.make_async_remote_copy(
            src_ref=src,
            dst_ref=dst,
            send_sem=send,
            recv_sem=recv,
            device_id={"ep": flip(ep, ep_bits), "tp": flip(tp, tp_bits)},
            device_id_type=pl.DeviceIdType.MESH,
        )

    loads = {
        name: pltpu.make_async_copy(a, b, load_sem.at[i])
        for i, (name, a, b) in enumerate(
            [
                ("expert", expert_hbm, expert_in),
                ("key", key_hbm, key),
                ("value", value_hbm, kv_all.at[pl.ds(0, local_rows), pl.ds(HEAD, HEAD)]),
                ("query", query_hbm, query),
                ("gate", gate_hbm, gate),
                ("up", up_hbm, up),
                ("down", down_hbm, down),
                ("out", out_w_hbm, out_w),
            ]
        )
    }
    for load in loads.values():
        load.start()

    def settle(name):
        if name in loads:
            loads.pop(name).wait()

    barrier = pltpu.get_barrier_semaphore()
    peers = [(j, 0) for j in range(1, n)] + [(0, 1), (0, 2)]
    for ep_bits, tp_bits in peers:
        pl.semaphore_signal(
            barrier,
            inc=1,
            device_id={"ep": flip(ep, ep_bits), "tp": flip(tp, tp_bits)},
            device_id_type=pl.DeviceIdType.MESH,
        )

    kv_stages = []
    held = [0]
    bit = n // 2
    while bit >= 1:
        kv_stages.append(
            [
                remote(
                    at(kv_all, block * local_rows, local_rows),
                    at(kv_all, (block + bit) * local_rows, local_rows),
                    kv_send.at[block + bit],
                    kv_recv.at[block + bit],
                    bit,
                    0,
                )
                for block in held
            ]
        )
        held = held + [block + bit for block in held]
        bit //= 2

    kv_last = list(kv_stages[-1])

    def place(slot, which):
        return (4 * slot + which) * cap

    dispatch, to_core, to_chip, relay = [], [], [], []
    p_core, p_chip, give_back = [], [], []
    for j in range(n):
        own = at(rows, place(j, 0), cap)
        dispatch.append(
            None
            if j == 0
            else remote(at(outg, j * cap, cap), own, disp_send.at[j], disp_recv.at[j], j, 0)
        )
        to_core.append(
            remote(own, at(rows, place(j, 2), cap), core_send.at[j], core_recv.at[j], 0, 1)
        )
        to_chip.append(
            remote(own, at(rows, place(j, 1), cap), chip_send.at[j], chip_recv.at[j], 0, 2)
        )
        relay.append(
            remote(
                at(rows, place(j, 1), cap),
                at(rows, place(j, 3), cap),
                relay_send.at[j],
                relay_recv.at[j],
                0,
                1,
            )
        )
        p_core.append(
            remote(
                at(part, place(j, 2), 2 * cap),
                at(part_in, 2 * j * cap, 2 * cap),
                pcore_send.at[j],
                pcore_recv.at[j],
                0,
                1,
            )
        )
        p_chip.append(
            remote(
                at(part_sum, j * cap, cap),
                at(part_xin, j * cap, cap),
                pchip_send.at[j],
                pchip_recv.at[j],
                0,
                2,
            )
        )
        give_back.append(
            None
            if j == 0
            else remote(
                at(final, j * cap, cap),
                at(ret, j * cap, cap),
                ret_send.at[j],
                ret_recv.at[j],
                j,
                0,
            )
        )

    def route():
        settle("expert")
        normed = rms_scale(expert_in[...].astype(f32), expert_gain_ref[...]).astype(bf16)
        number = lax.broadcasted_iota(jnp.int32, (n, tok_rows), 0)
        number = jnp.bitwise_xor(number, ep.astype(jnp.int32))
        chosen = jnp.zeros((n, tok_rows), f32)
        weight = jnp.zeros((n, tok_rows), f32)
        for k in range(routes_ref.shape[0]):
            same = routes_ref[k : k + 1, :] == number
            chosen = jnp.where(same, 1.0, chosen)
            weight = jnp.where(same, route_weight_ref[k : k + 1, :], weight)
        earlier = (
            lax.broadcasted_iota(jnp.int32, (tok_rows, tok_rows), 0)
            < lax.broadcasted_iota(jnp.int32, (tok_rows, tok_rows), 1)
        ).astype(f32)
        rank = jnp.dot(chosen, earlier, preferred_element_type=f32)
        rank = jnp.where(chosen > 0.5, rank, -1.0)
        slot = lax.broadcasted_iota(jnp.int32, (cap, tok_rows), 0).astype(f32)
        picks = []
        for j in range(n):
            taken = slot == rank[j : j + 1, :]
            picks.append(jnp.where(taken, 1.0, 0.0))
            slot_weight[j * cap : (j + 1) * cap, :] = jnp.where(taken, weight[j : j + 1, :], 0.0)
        pick = jnp.concatenate(picks, axis=0).astype(bf16)
        out = jnp.dot(pick, normed, preferred_element_type=f32).astype(bf16)
        rows[0:cap, :] = out[0:cap, :]
        outg[cap:, :] = out[cap:, :]

    def turned(values_in, gain):
        field = rms_scale(values_in.astype(f32), gain)
        lane = lax.broadcasted_iota(jnp.int32, field.shape, 1)
        first = jnp.bitwise_and(lane, HEAD // 2 - 1) < HEAD // 4
        partner = jnp.where(
            first,
            pltpu.roll(field, HEAD - HEAD // 4, axis=1),
            pltpu.roll(field, HEAD // 4, axis=1),
        )
        pieces = []
        for r in range(grid_rows):
            span = slice(r * GRID_W, (r + 1) * GRID_W)
            line = pl.ds(ep * grid_rows + r, 1)
            cosine = row_cos_ref[line, :] + col_cos_ref[...]
            sine = row_sin_ref[line, :] + col_sin_ref[...]
            pieces.append(field[span] * cosine + partner[span] * sine)
        return jnp.concatenate(pieces, axis=0).astype(bf16)

    def turn_keys():
        settle("key")
        kv_all[0:local_rows, 0:HEAD] = turned(key[...], key_gain_ref[...])
        settle("value")

    def forward(j):
        if j:
            dispatch[j].wait_recv()
        to_chip[j].start()
        to_core[j].start()

    def pass_on(j):
        to_chip[j].wait_recv()
        relay[j].start()

    def compute(js):
        for name in ("gate", "up", "down"):
            settle(name)
        for j in js:
            to_core[j].wait_recv()
            relay[j].wait_recv()
        span = pl.ds(place(js[0], 0), 4 * len(js) * cap)
        taken = rows[span, :]
        hidden = clamped_unit(
            jnp.dot(taken, gate[...], preferred_element_type=f32),
            jnp.dot(taken, up[...], preferred_element_type=f32),
        )
        part[span, :] = jnp.dot(hidden, down[...], preferred_element_type=f32).astype(bf16)
        for j in js:
            p_core[j].start()

    def wide(ref, start, size):
        return ref[pl.ds(start, size), :].astype(f32)

    def reduce_core(j):
        p_core[j].wait_recv()
        part_sum[pl.ds(j * cap, cap), :] = (
            wide(part, place(j, 1), cap) + wide(part_in, (2 * j + 1) * cap, cap)
        ).astype(bf16)
        p_chip[j].start()

    def reduce_chip(j):
        p_chip[j].wait_recv()
        summed = (
            wide(part, place(j, 0), cap)
            + wide(part_in, 2 * j * cap, cap)
            + wide(part_xin, j * cap, cap)
        ).astype(bf16)
        if j == 0:
            ret[pl.ds(0, cap), :] = summed
        else:
            final[pl.ds(j * cap, cap), :] = summed
            give_back[j].start()

    def kv_stage(s):
        if s:
            for copy in kv_stages[s - 1]:
                copy.wait_recv()
        for copy in kv_stages[s]:
            copy.start()

    def attend(head):
        settle("query")
        while kv_last:
            kv_last.pop().wait_recv()
        column = slice(head * HEAD, (head + 1) * HEAD)
        scores = lax.dot_general(
            turned(query[:, column], query_gain_ref[...]),
            kv_all[:, :HEAD],
            (((1,), (1,)), ((), ())),
            preferred_element_type=f32,
        ) * (HEAD ** (-0.5))
        expo = jnp.exp(scores - jnp.max(scores, axis=-1, keepdims=True))
        total = jnp.sum(expo, axis=-1, keepdims=True)
        summed = jnp.dot(expo.astype(bf16), kv_all[:, HEAD:], preferred_element_type=f32)
        att[:, column] = (summed / total).astype(bf16)

    def block_of(bits):
        return pl.multiple_of(flip(tp, bits) * share, share)

    mix_core = [
        remote(
            at(proj, block_of(1 + 2 * i), share),
            at(proj_in, i * share, share),
            mix_send.at[i],
            mix_recv.at[i],
            0,
            1,
        )
        for i in range(2)
    ]
    mix_chip = remote(proj_sum, proj_xin, mix_send.at[2], mix_recv.at[2], 0, 2)

    def project():
        settle("out")
        proj[...] = jnp.dot(att[...], out_w[...], preferred_element_type=f32).astype(bf16)
        for copy in mix_core:
            copy.start()

    def mix_reduce():
        for copy in mix_core:
            copy.wait_recv()
        proj_sum[...] = (wide(proj, block_of(2), share) + wide(proj_in, share, share)).astype(bf16)
        mix_chip.start()

    def mix_finish():
        mix_chip.wait_recv()
        summed = (
            wide(proj, block_of(0), share)
            + wide(proj_in, 0, share)
            + proj_xin[...].astype(f32)
        )
        mixer_out_ref[...] = rms_scale(summed, mixer_gain_ref[...]).astype(bf16)

    def finish():
        for copy in give_back[1:]:
            copy.wait_recv()
        rest = slot_weight[...]
        combined = jnp.zeros((tok_rows, width), f32)
        for _ in range(3):
            piece = rest.astype(bf16)
            rest = rest - piece.astype(f32)
            combined = combined + lax.dot_general(
                piece, ret[...], (((0,), (0,)), ((), ())), preferred_element_type=f32
            )
        expert_out_ref[...] = rms_scale(combined, ffn_gain_ref[...]).astype(bf16)

    actions = {
        "F": forward,
        "D": lambda j: dispatch[j].start(),
        "R": pass_on,
        "P": reduce_core,
        "G": reduce_chip,
        "K": kv_stage,
        "A": attend,
    }
    single = {
        "KR": turn_keys,
        "W": lambda: None,
        "O": project,
        "M": mix_reduce,
        "N": mix_finish,
        "E": finish,
    }
    with jax.named_scope("route"):
        route()
    with jax.named_scope("barrier"):
        pl.semaphore_wait(barrier, len(peers))
    for step in STEPS:
        with jax.named_scope(step):
            if step in single:
                single[step]()
            elif step[0] == "C":
                compute([int(c) for c in step[1:]])
            else:
                actions[step[0]](int(step[1:]))
    with jax.named_scope("drain"):
        for copy in (
            [c for stage in kv_stages for c in stage]
            + dispatch[1:]
            + to_core
            + to_chip
            + relay
            + p_core
            + p_chip
            + give_back[1:]
            + mix_core
            + [mix_chip]
        ):
            copy.wait_send()


def fused_local(
    queries,
    keys,
    values,
    query_gain,
    key_gain,
    out_weight,
    mixer_gain,
    expert_in,
    routes,
    route_weights,
    expert_gain,
    gate_w,
    up_w,
    down_w,
    ffn_out_gain,
):
    n = lax.axis_size("ep")
    local_rows, query_width = queries.shape
    tok_rows, width = expert_in.shape
    cap = capacity_of(tok_rows, routes.shape[1], n)
    hidden = gate_w.shape[2]
    share = local_rows // 4
    vmem = pl.BlockSpec(memory_space=pltpu.VMEM)
    anywhere = pl.BlockSpec(memory_space=pl.ANY)
    bf16, f32 = jnp.bfloat16, jnp.float32
    dma = pltpu.SemaphoreType.DMA

    return pl.pallas_call(
        fused_kernel,
        out_shape=(
            jax.ShapeDtypeStruct((share, width), bf16),
            jax.ShapeDtypeStruct((tok_rows, width), bf16),
        ),
        in_specs=[anywhere] * 8 + [vmem] * 11,
        out_specs=(vmem, vmem),
        scratch_shapes=[
            pltpu.VMEM((local_rows, query_width), bf16),
            pltpu.VMEM((local_rows, HEAD), bf16),
            pltpu.VMEM((tok_rows, width), bf16),
            pltpu.VMEM((query_width, width), bf16),
            pltpu.VMEM((width, hidden), bf16),
            pltpu.VMEM((width, hidden), bf16),
            pltpu.VMEM((hidden, width), bf16),
            pltpu.VMEM((n * local_rows, 2 * HEAD), bf16),
            pltpu.VMEM((local_rows, query_width), bf16),
            pltpu.VMEM((local_rows, width), bf16),
            pltpu.VMEM((2 * share, width), bf16),
            pltpu.VMEM((share, width), bf16),
            pltpu.VMEM((share, width), bf16),
            pltpu.VMEM((n * cap, width), bf16),
            pltpu.VMEM((n * cap, tok_rows), f32),
            pltpu.VMEM((4 * n * cap, width), bf16),
            pltpu.VMEM((4 * n * cap, width), bf16),
            pltpu.VMEM((2 * n * cap, width), bf16),
            pltpu.VMEM((n * cap, width), bf16),
            pltpu.VMEM((n * cap, width), bf16),
            pltpu.VMEM((n * cap, width), bf16),
            pltpu.VMEM((n * cap, width), bf16),
            dma((8,)),
        ]
        + [dma((n,))] * 16
        + [dma((3,))] * 2,
        compiler_params=pltpu.CompilerParams(
            collective_id=0, has_side_effects=True, vmem_limit_bytes=60 * 2**20
        ),
    )(
        queries,
        keys,
        values,
        expert_in,
        out_weight,
        gate_w[0],
        up_w[0],
        down_w[0],
        query_gain[None],
        key_gain[None],
        mixer_gain[None],
        expert_gain[None],
        ffn_out_gain[None],
        routes.T,
        route_weights.T,
        *rope_tables(n * local_rows // GRID_W),
    )


def local(
    queries,
    keys,
    values,
    query_gain,
    key_gain,
    out_weight,
    mixer_gain,
    expert_in,
    routes,
    route_weights,
    expert_gain,
    gate_w,
    up_w,
    down_w,
    ffn_out_gain,
):
    if fused_fits(queries, keys, expert_in, routes, gate_w):
        return fused_local(
            queries, keys, values, query_gain, key_gain, out_weight, mixer_gain, expert_in, routes,
            route_weights, expert_gain, gate_w, up_w, down_w, ffn_out_gain,
        )
    mixer_out = mixer_half(queries, keys, values, query_gain, key_gain, out_weight, mixer_gain)
    expert_out = expert_half(
        expert_in, routes, route_weights, expert_gain, gate_w, up_w, down_w, ffn_out_gain
    )
    return (mixer_out, expert_out)


def solution(mesh):
    in_specs = (
        P("ep", "tp"),
        P("ep", "tp"),
        P("ep", "tp"),
        P(),
        P(),
        P("tp", None),
        P(),
        P(("ep", "tp"), None),
        P(("ep", "tp"), None),
        P(("ep", "tp"), None),
        P(),
        P("ep", None, "tp"),
        P("ep", None, "tp"),
        P("ep", "tp", None),
        P(),
    )
    out_specs = (P(("ep", "tp"), None), P(("ep", "tp"), None))
    return jax.shard_map(local, mesh=mesh, in_specs=in_specs, out_specs=out_specs, check_vma=False)
```

```python
import jax
import jax.numpy as jnp
import numpy as np
from jax import lax
from jax.experimental import pallas as pl
from jax.experimental.pallas import tpu as pltpu
from jax.sharding import PartitionSpec as P

HEAD = 128
GRID_W = 64


norm_eps = 1e-06
rope_base = 10000.0
clamp_limit = 7.0
sigmoid_slope = 1.702


def rms_scale(values_in, gain):
    return (
        values_in
        * lax.rsqrt(jnp.mean(values_in * values_in, axis=-1, keepdims=True) + norm_eps)
        * gain
    )


def turn_pair(halfpart, cosine, sine):
    first_part, second_part = jnp.split(halfpart, 2, axis=-1)
    return jnp.concatenate(
        [first_part * cosine - second_part * sine, second_part * cosine + first_part * sine],
        axis=-1,
    )


def grid_rotate(field, position):
    half_width = field.shape[-1] // 2
    inverse = rope_base ** (-jnp.arange(0, half_width, 2, dtype=jnp.float32) / half_width)
    grid_row = (position // GRID_W).astype(jnp.float32)
    grid_col = (position % GRID_W).astype(jnp.float32)
    row_angle = (grid_row[:, None] * inverse[None, :])[:, None, :]
    col_angle = (grid_col[:, None] * inverse[None, :])[:, None, :]
    return jnp.concatenate(
        [
            turn_pair(field[..., :half_width], jnp.cos(row_angle), jnp.sin(row_angle)),
            turn_pair(field[..., half_width:], jnp.cos(col_angle), jnp.sin(col_angle)),
        ],
        axis=-1,
    )


def clamped_unit(gate_pre, up_pre):
    gate_cut = jnp.minimum(gate_pre, clamp_limit)
    up_cut = jnp.clip(up_pre, -clamp_limit, clamp_limit)
    return ((up_cut + 1.0) * gate_cut * jax.nn.sigmoid(sigmoid_slope * gate_cut)).astype(
        jnp.bfloat16
    )


def mixer_half(queries, keys, values, query_gain, key_gain, out_weight, mixer_gain):
    local_rows = queries.shape[0]
    kv_local = keys.shape[1] // HEAD
    group_size = queries.shape[1] // HEAD // kv_local
    position = lax.axis_index("ep") * local_rows + jnp.arange(local_rows, dtype=jnp.int32)
    query_f = queries.astype(jnp.float32).reshape(local_rows, kv_local * group_size, HEAD)
    query_norm = grid_rotate(rms_scale(query_f, query_gain), position).astype(jnp.bfloat16)
    query_norm = query_norm.reshape(local_rows, kv_local, group_size, HEAD)
    key_f = keys.astype(jnp.float32).reshape(local_rows, kv_local, HEAD)
    key_norm = grid_rotate(rms_scale(key_f, key_gain), position).astype(jnp.bfloat16)
    key_norm = key_norm.reshape(local_rows, kv_local * HEAD)
    score_scale = HEAD ** (-0.5)
    initial = (
        jnp.full((kv_local, group_size, local_rows), -1e30, jnp.float32),
        jnp.zeros((kv_local, group_size, local_rows), jnp.float32),
        jnp.zeros((kv_local, group_size, local_rows, HEAD), jnp.float32),
    )
    key_piece = lax.all_gather(key_norm, "ep", axis=0, tiled=True)
    value_piece = lax.all_gather(values, "ep", axis=0, tiled=True)
    piece_rows = key_piece.shape[0]
    block_rows = 1
    for candidate in range(min(piece_rows, 1024), 0, -1):
        if piece_rows % candidate == 0:
            block_rows = candidate
            break
    key_blocks = key_piece.reshape(piece_rows // block_rows, block_rows, kv_local, HEAD)
    value_blocks = value_piece.reshape(piece_rows // block_rows, block_rows, kv_local, HEAD)

    def one_block(state, blocks_in):
        running_max, running_total, weighted = state
        key_block, value_block = blocks_in
        scores = (
            jnp.einsum("qhgd,khd->hgqk", query_norm, key_block, preferred_element_type=jnp.float32)
            * score_scale
        )
        new_max = jnp.maximum(running_max, jnp.max(scores, axis=-1))
        factor = jnp.exp(running_max - new_max)
        expo = jnp.exp(scores - new_max[..., None])
        new_total = running_total * factor + jnp.sum(expo, axis=-1)
        new_weighted = weighted * factor[..., None] + jnp.einsum(
            "hgqk,khd->hgqd",
            expo.astype(jnp.bfloat16),
            value_block,
            preferred_element_type=jnp.float32,
        )
        return ((new_max, new_total, new_weighted), None)

    state_out, unused = lax.scan(one_block, initial, (key_blocks, value_blocks))
    final_max, final_total, weighted = state_out
    attended = (weighted / final_total[..., None]).astype(jnp.bfloat16)
    attended = jnp.transpose(attended, (2, 0, 1, 3)).reshape(
        local_rows, kv_local * group_size * HEAD
    )
    share_rows = local_rows // lax.axis_size("tp")
    selected = lax.slice_in_dim(attended, 0, lax.axis_size("tp") * share_rows, axis=0)
    projected = lax.psum_scatter(
        jnp.dot(selected, out_weight, preferred_element_type=jnp.float32).astype(jnp.bfloat16),
        "tp",
        scatter_dimension=0,
        tiled=True,
    ).astype(jnp.float32)
    return rms_scale(projected, mixer_gain).astype(jnp.bfloat16)


def expert_half(expert_in, routes, route_weights, expert_gain, gate_w, up_w, down_w, ffn_out_gain):
    tok_rows = expert_in.shape[0]
    model_width = expert_in.shape[1]
    top_count = routes.shape[1]
    expert_count = lax.axis_size("ep")
    capacity = max(2, (3 * tok_rows * top_count + 2 * expert_count - 1) // (2 * expert_count))
    normed = rms_scale(expert_in.astype(jnp.float32), expert_gain).astype(jnp.bfloat16)
    pair_expert = routes.reshape(-1)
    pair_count = pair_expert.shape[0]
    one_hot = (pair_expert[:, None] == jnp.arange(expert_count, dtype=jnp.int32)[None, :]).astype(
        jnp.int32
    )
    pair_rank = jnp.sum(jnp.cumsum(one_hot, axis=0) * one_hot, axis=1) - 1
    pair_slot = pair_expert * capacity + pair_rank
    slot_pair = (
        jnp.full((expert_count * capacity,), pair_count, jnp.int32)
        .at[pair_slot]
        .set(jnp.arange(pair_count, dtype=jnp.int32))
    )
    padded = jnp.concatenate([normed, jnp.zeros((1, model_width), jnp.bfloat16)], axis=0)
    outgoing = padded[slot_pair // top_count].reshape(expert_count, capacity, model_width)
    gate_local = gate_w[0]
    up_local = up_w[0]
    down_local = down_w[0]
    arrived = lax.all_to_all(outgoing, "ep", split_axis=0, concat_axis=0, tiled=True)
    flat_rows = arrived.reshape(-1, model_width)
    shard_rows = lax.all_gather(flat_rows, "tp", axis=0, tiled=True)
    hidden = clamped_unit(
        jnp.dot(shard_rows, gate_local, preferred_element_type=jnp.float32),
        jnp.dot(shard_rows, up_local, preferred_element_type=jnp.float32),
    )
    selected = lax.slice_in_dim(hidden, 0, lax.axis_size("tp") * flat_rows.shape[0], axis=0)
    result = lax.psum_scatter(
        jnp.dot(selected, down_local, preferred_element_type=jnp.float32).astype(jnp.bfloat16),
        "tp",
        scatter_dimension=0,
        tiled=True,
    )
    finished = result.reshape(arrived.shape)
    returned = lax.all_to_all(finished, "ep", split_axis=0, concat_axis=0, tiled=True)
    pair_result = returned.reshape(-1, model_width)[pair_slot].reshape(
        tok_rows, top_count, model_width
    )
    combined = jnp.einsum("tk,tkd->td", route_weights, pair_result.astype(jnp.float32))
    return rms_scale(combined, ffn_out_gain).astype(jnp.bfloat16)


def flip(index, bits):
    power = 1
    while power <= bits:
        if bits & power:
            index = index + power - 2 * power * lax.rem(lax.div(index, power), 2)
        power *= 2
    return index


def capacity_of(tok_rows, top_count, expert_count):
    return max(2, (3 * tok_rows * top_count + 2 * expert_count - 1) // (2 * expert_count))


def fused_fits(queries, keys, expert_in, routes, gate_w):
    n_ep, n_tp = lax.axis_size("ep"), lax.axis_size("tp")
    rows = queries.shape[0]
    capacity = capacity_of(expert_in.shape[0], routes.shape[1], n_ep)
    width = expert_in.shape[1]
    hidden = gate_w.shape[2]
    slots = n_ep * capacity
    held = 2 * width * slots * 14 + 6 * width * hidden * 4 + 4 * rows * rows * n_ep
    return (
        n_tp == 4
        and n_ep >= 4
        and n_ep & (n_ep - 1) == 0
        and keys.shape[1] == HEAD
        and capacity % 16 == 0
        and rows % (16 * n_tp) == 0
        and rows % GRID_W == 0
        and queries.shape[1] % HEAD == 0
        and expert_in.shape[0] % 16 == 0
        and held < 56 * 2**20
    )


STEPS = (
    "D4", "D2", "D1", "KR", "F0", "F1", "D3", "R0", "K0", "D5", "F2", "F4", "K1", "F3", "F5",
    "D7", "R1", "R4", "C4", "K2", "R2", "R3", "P4", "C3", "P3", "F7", "D6", "R5", "C5", "C1",
    "P5", "G3", "C2", "A2", "G4", "R7", "F6", "G5", "A0", "P2", "A1", "C7", "R6", "C0", "P7",
    "A3", "C6", "P1", "P6", "O", "G7", "P0", "M", "G1", "G2", "G6", "G0", "Q", "N", "E",
)


def turn_table(grid_rows):
    half = HEAD // 2
    lane = np.arange(HEAD)
    inverse = rope_base ** (-2.0 * (lane % (half // 2)) / half)
    sign = np.where(lane % half < half // 2, -1.0, 1.0)
    row = np.arange(grid_rows)[:, None] * inverse[None, :]
    col = np.arange(GRID_W)[:, None] * inverse[None, :]
    low = (lane < half)[None, :]
    tables = (
        np.where(low, 0.0, np.cos(col)),
        np.where(low, 0.0, np.sin(col) * sign),
        np.where(low, np.cos(row), 0.0),
        np.where(low, np.sin(row) * sign, 0.0),
    )
    return jnp.asarray(np.concatenate(tables).astype(np.float32))


def fused_kernel(
    query_hbm,
    key_hbm,
    value_hbm,
    expert_hbm,
    out_w_hbm,
    gate_hbm,
    up_hbm,
    down_hbm,
    expert_gain_hbm,
    routes_hbm,
    route_weight_hbm,
    query_gain_hbm,
    key_gain_hbm,
    turn_hbm,
    mixer_gain_hbm,
    ffn_gain_hbm,
    mixer_out_ref,
    expert_out_ref,
    expert_gain_ref,
    routes_ref,
    route_weight_ref,
    query_gain_ref,
    key_gain_ref,
    turn_ref,
    mixer_gain_ref,
    ffn_gain_ref,
    query,
    key,
    expert_in,
    out_w,
    gate,
    up,
    down,
    kv_all,
    att,
    proj,
    proj_in,
    proj_sum,
    proj_xin,
    outg,
    slot_weight,
    rows,
    part,
    part_in,
    part_sum,
    part_xin,
    final,
    ret,
    combined,
    load_sem,
    kv_send,
    kv_recv,
    disp_send,
    disp_recv,
    core_send,
    core_recv,
    chip_send,
    chip_recv,
    relay_send,
    relay_recv,
    pcore_send,
    pcore_recv,
    pchip_send,
    pchip_recv,
    ret_send,
    ret_recv,
    mix_send,
    mix_recv,
):
    tok_rows, width = expert_in.shape
    n = disp_send.shape[0]
    cap = ret.shape[0] // n
    local_rows = key.shape[0]
    share = local_rows // 4
    heads = query.shape[1] // HEAD
    grid_rows = local_rows // GRID_W
    bf16, f32 = jnp.bfloat16, jnp.float32
    ep, tp = lax.axis_index("ep"), lax.axis_index("tp")

    def at(ref, start, size):
        return ref.at[pl.ds(start, size), :]

    def remote(src, dst, send, recv, ep_bits, tp_bits):
        return pltpu.make_async_remote_copy(
            src_ref=src,
            dst_ref=dst,
            send_sem=send,
            recv_sem=recv,
            device_id={"ep": flip(ep, ep_bits), "tp": flip(tp, tp_bits)},
            device_id_type=pl.DeviceIdType.MESH,
        )

    barrier = pltpu.get_barrier_semaphore()
    peers = [(j, 0) for j in range(1, n)] + [(0, 1), (0, 2)]
    for ep_bits, tp_bits in peers:
        pl.semaphore_signal(
            barrier,
            inc=1,
            device_id={"ep": flip(ep, ep_bits), "tp": flip(tp, tp_bits)},
            device_id_type=pl.DeviceIdType.MESH,
        )

    loads = {
        name: pltpu.make_async_copy(a, b, load_sem.at[i])
        for i, (name, a, b) in enumerate(
            [
                ("expert", expert_hbm, expert_in),
                ("routes", routes_hbm, routes_ref),
                ("route_weight", route_weight_hbm, route_weight_ref),
                ("expert_gain", expert_gain_hbm, expert_gain_ref),
                ("query_gain", query_gain_hbm, query_gain_ref),
                ("key_gain", key_gain_hbm, key_gain_ref),
                ("turn", turn_hbm, turn_ref),
                ("key", key_hbm, key),
                ("value", value_hbm, kv_all.at[pl.ds(0, local_rows), pl.ds(HEAD, HEAD)]),
                ("query", query_hbm, query),
                ("gate", gate_hbm, gate),
                ("up", up_hbm, up),
                ("down", down_hbm, down),
                ("out", out_w_hbm, out_w),
                ("mixer_gain", mixer_gain_hbm, mixer_gain_ref),
                ("ffn_gain", ffn_gain_hbm, ffn_gain_ref),
            ]
        )
    }

    for load in loads.values():
        load.start()

    def settle(*names):
        for name in names:
            if name in loads:
                loads.pop(name).wait()

    kv_stages = []
    held = [0]
    bit = n // 2
    while bit >= 1:
        kv_stages.append(
            [
                remote(
                    at(kv_all, block * local_rows, local_rows),
                    at(kv_all, (block + bit) * local_rows, local_rows),
                    kv_send.at[block + bit],
                    kv_recv.at[block + bit],
                    bit,
                    0,
                )
                for block in held
            ]
        )
        held = held + [block + bit for block in held]
        bit //= 2

    kv_last = list(kv_stages[-1])

    def place(slot, which):
        return (4 * slot + which) * cap

    dispatch, to_core, to_chip, relay = [], [], [], []
    p_core, p_chip, give_back = [], [], []
    for j in range(n):
        own = at(rows, place(j, 0), cap)
        dispatch.append(
            None
            if j == 0
            else remote(at(outg, j * cap, cap), own, disp_send.at[j], disp_recv.at[j], j, 0)
        )
        to_core.append(
            remote(own, at(rows, place(j, 2), cap), core_send.at[j], core_recv.at[j], 0, 1)
        )
        to_chip.append(
            remote(own, at(rows, place(j, 1), cap), chip_send.at[j], chip_recv.at[j], 0, 2)
        )
        relay.append(
            remote(
                at(rows, place(j, 1), cap),
                at(rows, place(j, 3), cap),
                relay_send.at[j],
                relay_recv.at[j],
                0,
                1,
            )
        )
        p_core.append(
            remote(
                at(part, place(j, 2), 2 * cap),
                at(part_in, 2 * j * cap, 2 * cap),
                pcore_send.at[j],
                pcore_recv.at[j],
                0,
                1,
            )
        )
        p_chip.append(
            remote(
                at(part_sum, j * cap, cap),
                at(part_xin, j * cap, cap),
                pchip_send.at[j],
                pchip_recv.at[j],
                0,
                2,
            )
        )
        give_back.append(
            None
            if j == 0
            else remote(
                at(final, j * cap, cap),
                at(ret, j * cap, cap),
                ret_send.at[j],
                ret_recv.at[j],
                j,
                0,
            )
        )

    def route():
        settle("routes", "route_weight")
        number = lax.broadcasted_iota(jnp.int32, (n, tok_rows), 0)
        number = jnp.bitwise_xor(number, ep.astype(jnp.int32))
        chosen = jnp.zeros((n, tok_rows), f32)
        weight = jnp.zeros((n, tok_rows), f32)
        for k in range(routes_ref.shape[0]):
            same = routes_ref[k : k + 1, :] == number
            chosen = jnp.where(same, 1.0, chosen)
            weight = jnp.where(same, route_weight_ref[k : k + 1, :], weight)
        earlier = (
            lax.broadcasted_iota(jnp.int32, (tok_rows, tok_rows), 0)
            < lax.broadcasted_iota(jnp.int32, (tok_rows, tok_rows), 1)
        ).astype(f32)
        rank = jnp.dot(chosen, earlier, preferred_element_type=f32)
        rank = jnp.where(chosen > 0.5, rank, -1.0)
        slot = lax.broadcasted_iota(jnp.int32, (cap, tok_rows), 0).astype(f32)
        picks = []
        for j in range(n):
            taken = slot == rank[j : j + 1, :]
            picks.append(jnp.where(taken, 1.0, 0.0))
            slot_weight[j * cap : (j + 1) * cap, :] = jnp.where(taken, weight[j : j + 1, :], 0.0)
        pick = jnp.concatenate(picks, axis=0).astype(bf16)
        settle("expert", "expert_gain")
        normed = rms_scale(expert_in[...].astype(f32), expert_gain_ref[...]).astype(bf16)
        out = jnp.dot(pick, normed, preferred_element_type=f32).astype(bf16)
        rows[0:cap, :] = out[0:cap, :]
        outg[cap:, :] = out[cap:, :]

    def turned(values_in, gain):
        field = rms_scale(values_in.astype(f32), gain)
        lane = lax.broadcasted_iota(jnp.int32, field.shape, 1)
        first = jnp.bitwise_and(lane, HEAD // 2 - 1) < HEAD // 4
        partner = jnp.where(
            first,
            pltpu.roll(field, HEAD - HEAD // 4, axis=1),
            pltpu.roll(field, HEAD // 4, axis=1),
        )
        pieces = []
        all_rows = n * grid_rows
        for r in range(grid_rows):
            span = slice(r * GRID_W, (r + 1) * GRID_W)
            line = 2 * GRID_W + ep * grid_rows + r
            cosine = turn_ref[pl.ds(line, 1), :] + turn_ref[0:GRID_W, :]
            sine = turn_ref[pl.ds(line + all_rows, 1), :] + turn_ref[GRID_W : 2 * GRID_W, :]
            pieces.append(field[span] * cosine + partner[span] * sine)
        return jnp.concatenate(pieces, axis=0).astype(bf16)

    def turn_keys():
        settle("key", "key_gain", "turn")
        kv_all[0:local_rows, 0:HEAD] = turned(key[...], key_gain_ref[...])
        settle("value")

    def forward(j):
        if j:
            dispatch[j].wait_recv()
        to_chip[j].start()
        to_core[j].start()

    def pass_on(j):
        to_chip[j].wait_recv()
        relay[j].start()

    def compute(js):
        for name in ("gate", "up", "down"):
            settle(name)
        for j in js:
            to_core[j].wait_recv()
            relay[j].wait_recv()
        span = pl.ds(place(js[0], 0), 4 * len(js) * cap)
        taken = rows[span, :]
        hidden = clamped_unit(
            jnp.dot(taken, gate[...], preferred_element_type=f32),
            jnp.dot(taken, up[...], preferred_element_type=f32),
        )
        part[span, :] = jnp.dot(hidden, down[...], preferred_element_type=f32).astype(bf16)
        for j in js:
            p_core[j].start()

    def wide(ref, start, size):
        return ref[pl.ds(start, size), :].astype(f32)

    def reduce_core(j):
        p_core[j].wait_recv()
        part_sum[pl.ds(j * cap, cap), :] = (
            wide(part, place(j, 1), cap) + wide(part_in, (2 * j + 1) * cap, cap)
        ).astype(bf16)
        p_chip[j].start()

    def reduce_chip(j):
        p_chip[j].wait_recv()
        summed = (
            wide(part, place(j, 0), cap)
            + wide(part_in, 2 * j * cap, cap)
            + wide(part_xin, j * cap, cap)
        ).astype(bf16)
        if j == 0:
            ret[pl.ds(0, cap), :] = summed
        else:
            final[pl.ds(j * cap, cap), :] = summed
            give_back[j].start()

    def kv_stage(s):
        if s:
            for copy in kv_stages[s - 1]:
                copy.wait_recv()
        for copy in kv_stages[s]:
            copy.start()

    def attend(head):
        settle("query", "query_gain", "turn")
        while kv_last:
            kv_last.pop().wait_recv()
        column = slice(head * HEAD, (head + 1) * HEAD)
        scores = lax.dot_general(
            turned(query[:, column], query_gain_ref[...]),
            kv_all[:, :HEAD],
            (((1,), (1,)), ((), ())),
            preferred_element_type=f32,
        ) * (HEAD ** (-0.5))
        expo = jnp.exp(scores - jnp.max(scores, axis=-1, keepdims=True))
        total = jnp.sum(expo, axis=-1, keepdims=True)
        summed = jnp.dot(expo.astype(bf16), kv_all[:, HEAD:], preferred_element_type=f32)
        att[:, column] = (summed / total).astype(bf16)

    def block_of(bits):
        return pl.multiple_of(flip(tp, bits) * share, share)

    mix_core = [
        remote(
            at(proj, block_of(1 + 2 * i), share),
            at(proj_in, i * share, share),
            mix_send.at[i],
            mix_recv.at[i],
            0,
            1,
        )
        for i in range(2)
    ]
    mix_chip = remote(proj_sum, proj_xin, mix_send.at[2], mix_recv.at[2], 0, 2)

    def project():
        settle("out")
        proj[...] = jnp.dot(att[...], out_w[...], preferred_element_type=f32).astype(bf16)
        for copy in mix_core:
            copy.start()

    def mix_reduce():
        for copy in mix_core:
            copy.wait_recv()
        proj_sum[...] = (wide(proj, block_of(2), share) + wide(proj_in, share, share)).astype(bf16)
        mix_chip.start()

    def mix_finish():
        mix_chip.wait_recv()
        settle("mixer_gain")
        summed = (
            wide(proj, block_of(0), share)
            + wide(proj_in, 0, share)
            + proj_xin[...].astype(f32)
        )
        mixer_out_ref[...] = rms_scale(summed, mixer_gain_ref[...]).astype(bf16)

    def weighted(start, size):
        rest = slot_weight[start : start + size, :]
        total = None
        for _ in range(3):
            piece = rest.astype(bf16)
            rest = rest - piece.astype(f32)
            term = lax.dot_general(
                piece,
                ret[start : start + size, :],
                (((0,), (0,)), ((), ())),
                preferred_element_type=f32,
            )
            total = term if total is None else total + term
        return total

    def gather():
        for copy in give_back[1:]:
            copy.wait_recv()
        combined[...] = weighted(cap, (n - 1) * cap)

    def finish():
        settle("ffn_gain")
        total = combined[...] + weighted(0, cap)
        expert_out_ref[...] = rms_scale(total, ffn_gain_ref[...]).astype(bf16)

    actions = {
        "F": forward,
        "D": lambda j: dispatch[j].start(),
        "R": pass_on,
        "P": reduce_core,
        "G": reduce_chip,
        "K": kv_stage,
        "A": attend,
    }
    single = {
        "KR": turn_keys,
        "O": project,
        "M": mix_reduce,
        "N": mix_finish,
        "Q": gather,
        "E": finish,
    }
    with jax.named_scope("route"):
        route()
    with jax.named_scope("barrier"):
        pl.semaphore_wait(barrier, len(peers))
    for step in STEPS:
        with jax.named_scope(step):
            if step in single:
                single[step]()
            elif step[0] == "C":
                compute([int(c) for c in step[1:]])
            else:
                actions[step[0]](int(step[1:]))
    with jax.named_scope("drain"):
        for copy in (
            [c for stage in kv_stages for c in stage]
            + dispatch[1:]
            + to_core
            + to_chip
            + relay
            + p_core
            + p_chip
            + give_back[1:]
            + mix_core
            + [mix_chip]
        ):
            copy.wait_send()


def fused_local(
    queries,
    keys,
    values,
    query_gain,
    key_gain,
    out_weight,
    mixer_gain,
    expert_in,
    routes,
    route_weights,
    expert_gain,
    gate_w,
    up_w,
    down_w,
    ffn_out_gain,
):
    n = lax.axis_size("ep")
    local_rows, query_width = queries.shape
    tok_rows, width = expert_in.shape
    cap = capacity_of(tok_rows, routes.shape[1], n)
    hidden = gate_w.shape[2]
    share = local_rows // 4
    table = turn_table(n * local_rows // GRID_W)
    vmem = pl.BlockSpec(memory_space=pltpu.VMEM)
    anywhere = pl.BlockSpec(memory_space=pl.ANY)
    bf16, f32 = jnp.bfloat16, jnp.float32
    dma = pltpu.SemaphoreType.DMA

    return pl.pallas_call(
        fused_kernel,
        out_shape=(
            pltpu.VMEM((share, width), bf16),
            pltpu.VMEM((tok_rows, width), bf16),
        ),
        in_specs=[anywhere] * 16,
        out_specs=(vmem, vmem),
        scratch_shapes=[
            pltpu.VMEM((1, width), f32),
            pltpu.VMEM((routes.shape[1], tok_rows), jnp.int32),
            pltpu.VMEM((routes.shape[1], tok_rows), f32),
            pltpu.VMEM((1, HEAD), f32),
            pltpu.VMEM((1, HEAD), f32),
            pltpu.VMEM(table.shape, f32),
            pltpu.VMEM((1, width), f32),
            pltpu.VMEM((1, width), f32),
            pltpu.VMEM((local_rows, query_width), bf16),
            pltpu.VMEM((local_rows, HEAD), bf16),
            pltpu.VMEM((tok_rows, width), bf16),
            pltpu.VMEM((query_width, width), bf16),
            pltpu.VMEM((width, hidden), bf16),
            pltpu.VMEM((width, hidden), bf16),
            pltpu.VMEM((hidden, width), bf16),
            pltpu.VMEM((n * local_rows, 2 * HEAD), bf16),
            pltpu.VMEM((local_rows, query_width), bf16),
            pltpu.VMEM((local_rows, width), bf16),
            pltpu.VMEM((2 * share, width), bf16),
            pltpu.VMEM((share, width), bf16),
            pltpu.VMEM((share, width), bf16),
            pltpu.VMEM((n * cap, width), bf16),
            pltpu.VMEM((n * cap, tok_rows), f32),
            pltpu.VMEM((4 * n * cap, width), bf16),
            pltpu.VMEM((4 * n * cap, width), bf16),
            pltpu.VMEM((2 * n * cap, width), bf16),
            pltpu.VMEM((n * cap, width), bf16),
            pltpu.VMEM((n * cap, width), bf16),
            pltpu.VMEM((n * cap, width), bf16),
            pltpu.VMEM((n * cap, width), bf16),
            pltpu.VMEM((tok_rows, width), f32),
            dma((16,)),
        ]
        + [dma((n,))] * 16
        + [dma((3,))] * 2,
        compiler_params=pltpu.CompilerParams(
            collective_id=0, has_side_effects=True, vmem_limit_bytes=60 * 2**20
        ),
    )(
        queries,
        keys,
        values,
        expert_in,
        out_weight,
        gate_w[0],
        up_w[0],
        down_w[0],
        expert_gain[None],
        routes.T,
        route_weights.T,
        query_gain[None],
        key_gain[None],
        table,
        mixer_gain[None],
        ffn_out_gain[None],
    )


def local(
    queries,
    keys,
    values,
    query_gain,
    key_gain,
    out_weight,
    mixer_gain,
    expert_in,
    routes,
    route_weights,
    expert_gain,
    gate_w,
    up_w,
    down_w,
    ffn_out_gain,
):
    if fused_fits(queries, keys, expert_in, routes, gate_w):
        return fused_local(
            queries, keys, values, query_gain, key_gain, out_weight, mixer_gain, expert_in, routes,
            route_weights, expert_gain, gate_w, up_w, down_w, ffn_out_gain,
        )
    mixer_out = mixer_half(queries, keys, values, query_gain, key_gain, out_weight, mixer_gain)
    expert_out = expert_half(
        expert_in, routes, route_weights, expert_gain, gate_w, up_w, down_w, ffn_out_gain
    )
    return (mixer_out, expert_out)


def solution(mesh):
    in_specs = (
        P("ep", "tp"),
        P("ep", "tp"),
        P("ep", "tp"),
        P(),
        P(),
        P("tp", None),
        P(),
        P(("ep", "tp"), None),
        P(("ep", "tp"), None),
        P(("ep", "tp"), None),
        P(),
        P("ep", None, "tp"),
        P("ep", None, "tp"),
        P("ep", "tp", None),
        P(),
    )
    out_specs = (P(("ep", "tp"), None), P(("ep", "tp"), None))
    return jax.shard_map(local, mesh=mesh, in_specs=in_specs, out_specs=out_specs, check_vma=False)
```

```python
import jax
import jax.numpy as jnp
import numpy as np
from jax import lax
from jax.experimental import pallas as pl
from jax.experimental.pallas import tpu as pltpu
from jax.sharding import PartitionSpec as P

HEAD = 128
GRID_W = 64


norm_eps = 1e-06
rope_base = 10000.0
clamp_limit = 7.0
sigmoid_slope = 1.702


def rms_scale(values_in, gain):
    return (
        values_in
        * lax.rsqrt(jnp.mean(values_in * values_in, axis=-1, keepdims=True) + norm_eps)
        * gain
    )


def turn_pair(halfpart, cosine, sine):
    first_part, second_part = jnp.split(halfpart, 2, axis=-1)
    return jnp.concatenate(
        [first_part * cosine - second_part * sine, second_part * cosine + first_part * sine],
        axis=-1,
    )


def grid_rotate(field, position):
    half_width = field.shape[-1] // 2
    inverse = rope_base ** (-jnp.arange(0, half_width, 2, dtype=jnp.float32) / half_width)
    grid_row = (position // GRID_W).astype(jnp.float32)
    grid_col = (position % GRID_W).astype(jnp.float32)
    row_angle = (grid_row[:, None] * inverse[None, :])[:, None, :]
    col_angle = (grid_col[:, None] * inverse[None, :])[:, None, :]
    return jnp.concatenate(
        [
            turn_pair(field[..., :half_width], jnp.cos(row_angle), jnp.sin(row_angle)),
            turn_pair(field[..., half_width:], jnp.cos(col_angle), jnp.sin(col_angle)),
        ],
        axis=-1,
    )


def clamped_unit(gate_pre, up_pre):
    gate_cut = jnp.minimum(gate_pre, clamp_limit)
    up_cut = jnp.clip(up_pre, -clamp_limit, clamp_limit)
    return ((up_cut + 1.0) * gate_cut * jax.nn.sigmoid(sigmoid_slope * gate_cut)).astype(
        jnp.bfloat16
    )


def mixer_half(queries, keys, values, query_gain, key_gain, out_weight, mixer_gain):
    local_rows = queries.shape[0]
    kv_local = keys.shape[1] // HEAD
    group_size = queries.shape[1] // HEAD // kv_local
    position = lax.axis_index("ep") * local_rows + jnp.arange(local_rows, dtype=jnp.int32)
    query_f = queries.astype(jnp.float32).reshape(local_rows, kv_local * group_size, HEAD)
    query_norm = grid_rotate(rms_scale(query_f, query_gain), position).astype(jnp.bfloat16)
    query_norm = query_norm.reshape(local_rows, kv_local, group_size, HEAD)
    key_f = keys.astype(jnp.float32).reshape(local_rows, kv_local, HEAD)
    key_norm = grid_rotate(rms_scale(key_f, key_gain), position).astype(jnp.bfloat16)
    key_norm = key_norm.reshape(local_rows, kv_local * HEAD)
    score_scale = HEAD ** (-0.5)
    initial = (
        jnp.full((kv_local, group_size, local_rows), -1e30, jnp.float32),
        jnp.zeros((kv_local, group_size, local_rows), jnp.float32),
        jnp.zeros((kv_local, group_size, local_rows, HEAD), jnp.float32),
    )
    key_piece = lax.all_gather(key_norm, "ep", axis=0, tiled=True)
    value_piece = lax.all_gather(values, "ep", axis=0, tiled=True)
    piece_rows = key_piece.shape[0]
    block_rows = 1
    for candidate in range(min(piece_rows, 1024), 0, -1):
        if piece_rows % candidate == 0:
            block_rows = candidate
            break
    key_blocks = key_piece.reshape(piece_rows // block_rows, block_rows, kv_local, HEAD)
    value_blocks = value_piece.reshape(piece_rows // block_rows, block_rows, kv_local, HEAD)

    def one_block(state, blocks_in):
        running_max, running_total, weighted = state
        key_block, value_block = blocks_in
        scores = (
            jnp.einsum("qhgd,khd->hgqk", query_norm, key_block, preferred_element_type=jnp.float32)
            * score_scale
        )
        new_max = jnp.maximum(running_max, jnp.max(scores, axis=-1))
        factor = jnp.exp(running_max - new_max)
        expo = jnp.exp(scores - new_max[..., None])
        new_total = running_total * factor + jnp.sum(expo, axis=-1)
        new_weighted = weighted * factor[..., None] + jnp.einsum(
            "hgqk,khd->hgqd",
            expo.astype(jnp.bfloat16),
            value_block,
            preferred_element_type=jnp.float32,
        )
        return ((new_max, new_total, new_weighted), None)

    state_out, unused = lax.scan(one_block, initial, (key_blocks, value_blocks))
    final_max, final_total, weighted = state_out
    attended = (weighted / final_total[..., None]).astype(jnp.bfloat16)
    attended = jnp.transpose(attended, (2, 0, 1, 3)).reshape(
        local_rows, kv_local * group_size * HEAD
    )
    share_rows = local_rows // lax.axis_size("tp")
    selected = lax.slice_in_dim(attended, 0, lax.axis_size("tp") * share_rows, axis=0)
    projected = lax.psum_scatter(
        jnp.dot(selected, out_weight, preferred_element_type=jnp.float32).astype(jnp.bfloat16),
        "tp",
        scatter_dimension=0,
        tiled=True,
    ).astype(jnp.float32)
    return rms_scale(projected, mixer_gain).astype(jnp.bfloat16)


def expert_half(expert_in, routes, route_weights, expert_gain, gate_w, up_w, down_w, ffn_out_gain):
    tok_rows = expert_in.shape[0]
    model_width = expert_in.shape[1]
    top_count = routes.shape[1]
    expert_count = lax.axis_size("ep")
    capacity = max(2, (3 * tok_rows * top_count + 2 * expert_count - 1) // (2 * expert_count))
    normed = rms_scale(expert_in.astype(jnp.float32), expert_gain).astype(jnp.bfloat16)
    pair_expert = routes.reshape(-1)
    pair_count = pair_expert.shape[0]
    one_hot = (pair_expert[:, None] == jnp.arange(expert_count, dtype=jnp.int32)[None, :]).astype(
        jnp.int32
    )
    pair_rank = jnp.sum(jnp.cumsum(one_hot, axis=0) * one_hot, axis=1) - 1
    pair_slot = pair_expert * capacity + pair_rank
    slot_pair = (
        jnp.full((expert_count * capacity,), pair_count, jnp.int32)
        .at[pair_slot]
        .set(jnp.arange(pair_count, dtype=jnp.int32))
    )
    padded = jnp.concatenate([normed, jnp.zeros((1, model_width), jnp.bfloat16)], axis=0)
    outgoing = padded[slot_pair // top_count].reshape(expert_count, capacity, model_width)
    gate_local = gate_w[0]
    up_local = up_w[0]
    down_local = down_w[0]
    arrived = lax.all_to_all(outgoing, "ep", split_axis=0, concat_axis=0, tiled=True)
    flat_rows = arrived.reshape(-1, model_width)
    shard_rows = lax.all_gather(flat_rows, "tp", axis=0, tiled=True)
    hidden = clamped_unit(
        jnp.dot(shard_rows, gate_local, preferred_element_type=jnp.float32),
        jnp.dot(shard_rows, up_local, preferred_element_type=jnp.float32),
    )
    selected = lax.slice_in_dim(hidden, 0, lax.axis_size("tp") * flat_rows.shape[0], axis=0)
    result = lax.psum_scatter(
        jnp.dot(selected, down_local, preferred_element_type=jnp.float32).astype(jnp.bfloat16),
        "tp",
        scatter_dimension=0,
        tiled=True,
    )
    finished = result.reshape(arrived.shape)
    returned = lax.all_to_all(finished, "ep", split_axis=0, concat_axis=0, tiled=True)
    pair_result = returned.reshape(-1, model_width)[pair_slot].reshape(
        tok_rows, top_count, model_width
    )
    combined = jnp.einsum("tk,tkd->td", route_weights, pair_result.astype(jnp.float32))
    return rms_scale(combined, ffn_out_gain).astype(jnp.bfloat16)


def flip(index, bits):
    power = 1
    while power <= bits:
        if bits & power:
            index = index + power - 2 * power * lax.rem(lax.div(index, power), 2)
        power *= 2
    return index


def capacity_of(tok_rows, top_count, expert_count):
    return max(2, (3 * tok_rows * top_count + 2 * expert_count - 1) // (2 * expert_count))


def fused_fits(queries, keys, expert_in, routes, gate_w):
    n_ep, n_tp = lax.axis_size("ep"), lax.axis_size("tp")
    rows = queries.shape[0]
    capacity = capacity_of(expert_in.shape[0], routes.shape[1], n_ep)
    width = expert_in.shape[1]
    hidden = gate_w.shape[2]
    slots = n_ep * capacity
    held = 2 * width * slots * 14 + 6 * width * hidden * 4 + 4 * rows * rows * n_ep
    return (
        n_tp == 4
        and n_ep >= 4
        and n_ep & (n_ep - 1) == 0
        and keys.shape[1] == HEAD
        and capacity % 16 == 0
        and rows % (16 * n_tp) == 0
        and rows % GRID_W == 0
        and queries.shape[1] % HEAD == 0
        and expert_in.shape[0] % 16 == 0
        and held < 56 * 2**20
    )


STEPS = (
    "D4", "D2", "D1", "KR", "F0", "F1", "D3", "R0", "K0", "D5", "F4", "F2", "K1", "F3", "F5",
    "D7", "R1", "R4", "C4", "K2", "R2", "R3", "P4", "C3", "P3", "F7", "D6", "R5", "C5", "C1",
    "P5", "G3", "C2", "A2", "G4", "R7", "F6", "G5", "A0", "P2", "A1", "C7", "R6", "C0", "P7",
    "A3", "C6", "P1", "P6", "O", "G7", "P0", "M", "G1", "G2", "G6", "G0", "Q", "N", "E",
)


def turn_table(grid_rows):
    half = HEAD // 2
    lane = np.arange(HEAD)
    inverse = rope_base ** (-2.0 * (lane % (half // 2)) / half)
    sign = np.where(lane % half < half // 2, -1.0, 1.0)
    row = np.arange(grid_rows)[:, None] * inverse[None, :]
    col = np.arange(GRID_W)[:, None] * inverse[None, :]
    low = (lane < half)[None, :]
    tables = (
        np.where(low, 0.0, np.cos(col)),
        np.where(low, 0.0, np.sin(col) * sign),
        np.where(low, np.cos(row), 0.0),
        np.where(low, np.sin(row) * sign, 0.0),
    )
    return jnp.asarray(np.concatenate(tables).astype(np.float32))


def fused_kernel(
    query_hbm,
    key_hbm,
    value_hbm,
    expert_hbm,
    out_w_hbm,
    gate_hbm,
    up_hbm,
    down_hbm,
    expert_gain_hbm,
    routes_hbm,
    route_weight_hbm,
    query_gain_hbm,
    key_gain_hbm,
    turn_hbm,
    mixer_gain_hbm,
    ffn_gain_hbm,
    mixer_out_ref,
    expert_out_ref,
    expert_gain_ref,
    routes_ref,
    route_weight_ref,
    query_gain_ref,
    key_gain_ref,
    turn_ref,
    mixer_gain_ref,
    ffn_gain_ref,
    query,
    key,
    expert_in,
    out_w,
    gate,
    up,
    down,
    kv_all,
    att,
    proj,
    proj_in,
    proj_sum,
    proj_xin,
    outg,
    slot_weight,
    rows,
    part,
    part_in,
    part_sum,
    part_xin,
    final,
    ret,
    combined,
    load_sem,
    kv_send,
    kv_recv,
    disp_send,
    disp_recv,
    core_send,
    core_recv,
    chip_send,
    chip_recv,
    relay_send,
    relay_recv,
    pcore_send,
    pcore_recv,
    pchip_send,
    pchip_recv,
    ret_send,
    ret_recv,
    mix_send,
    mix_recv,
):
    tok_rows, width = expert_in.shape
    n = disp_send.shape[0]
    cap = ret.shape[0] // n
    local_rows = key.shape[0]
    share = local_rows // 4
    heads = query.shape[1] // HEAD
    grid_rows = local_rows // GRID_W
    bf16, f32 = jnp.bfloat16, jnp.float32
    ep, tp = lax.axis_index("ep"), lax.axis_index("tp")

    def at(ref, start, size):
        return ref.at[pl.ds(start, size), :]

    def remote(src, dst, send, recv, ep_bits, tp_bits):
        return pltpu.make_async_remote_copy(
            src_ref=src,
            dst_ref=dst,
            send_sem=send,
            recv_sem=recv,
            device_id={"ep": flip(ep, ep_bits), "tp": flip(tp, tp_bits)},
            device_id_type=pl.DeviceIdType.MESH,
        )

    barrier = pltpu.get_barrier_semaphore()
    peers = [(1 << b, 0) for b in range(n.bit_length() - 1)] + [(0, 1), (0, 2)]
    for ep_bits, tp_bits in peers:
        pl.semaphore_signal(
            barrier,
            inc=1,
            device_id={"ep": flip(ep, ep_bits), "tp": flip(tp, tp_bits)},
            device_id_type=pl.DeviceIdType.MESH,
        )

    loads = {
        name: pltpu.make_async_copy(a, b, load_sem.at[i])
        for i, (name, a, b) in enumerate(
            [
                ("expert", expert_hbm, expert_in),
                ("routes", routes_hbm, routes_ref),
                ("route_weight", route_weight_hbm, route_weight_ref),
                ("expert_gain", expert_gain_hbm, expert_gain_ref),
                ("query_gain", query_gain_hbm, query_gain_ref),
                ("key_gain", key_gain_hbm, key_gain_ref),
                ("turn", turn_hbm, turn_ref),
                ("key", key_hbm, key),
                ("value", value_hbm, kv_all.at[pl.ds(0, local_rows), pl.ds(HEAD, HEAD)]),
                ("query", query_hbm, query),
                ("gate", gate_hbm, gate),
                ("up", up_hbm, up),
                ("down", down_hbm, down),
                ("out", out_w_hbm, out_w),
                ("mixer_gain", mixer_gain_hbm, mixer_gain_ref),
                ("ffn_gain", ffn_gain_hbm, ffn_gain_ref),
            ]
        )
    }

    for load in loads.values():
        load.start()

    def settle(*names):
        for name in names:
            if name in loads:
                loads.pop(name).wait()

    kv_stages = []
    held = [0]
    bit = n // 2
    while bit >= 1:
        kv_stages.append(
            [
                remote(
                    at(kv_all, block * local_rows, local_rows),
                    at(kv_all, (block + bit) * local_rows, local_rows),
                    kv_send.at[block + bit],
                    kv_recv.at[block + bit],
                    bit,
                    0,
                )
                for block in held
            ]
        )
        held = held + [block + bit for block in held]
        bit //= 2

    kv_last = list(kv_stages[-1])

    def place(slot, which):
        return (4 * slot + which) * cap

    dispatch, to_core, to_chip, relay = [], [], [], []
    p_core, p_chip, give_back = [], [], []
    for j in range(n):
        own = at(rows, place(j, 0), cap)
        dispatch.append(
            None
            if j == 0
            else remote(at(outg, j * cap, cap), own, disp_send.at[j], disp_recv.at[j], j, 0)
        )
        to_core.append(
            remote(own, at(rows, place(j, 2), cap), core_send.at[j], core_recv.at[j], 0, 1)
        )
        to_chip.append(
            remote(own, at(rows, place(j, 1), cap), chip_send.at[j], chip_recv.at[j], 0, 2)
        )
        relay.append(
            remote(
                at(rows, place(j, 1), cap),
                at(rows, place(j, 3), cap),
                relay_send.at[j],
                relay_recv.at[j],
                0,
                1,
            )
        )
        p_core.append(
            remote(
                at(part, place(j, 2), 2 * cap),
                at(part_in, 2 * j * cap, 2 * cap),
                pcore_send.at[j],
                pcore_recv.at[j],
                0,
                1,
            )
        )
        p_chip.append(
            remote(
                at(part_sum, j * cap, cap),
                at(part_xin, j * cap, cap),
                pchip_send.at[j],
                pchip_recv.at[j],
                0,
                2,
            )
        )
        give_back.append(
            None
            if j == 0
            else remote(
                at(final, j * cap, cap),
                at(ret, j * cap, cap),
                ret_send.at[j],
                ret_recv.at[j],
                j,
                0,
            )
        )

    def route():
        settle("routes", "route_weight")
        number = lax.broadcasted_iota(jnp.int32, (n, tok_rows), 0)
        number = jnp.bitwise_xor(number, ep.astype(jnp.int32))
        chosen = jnp.zeros((n, tok_rows), f32)
        weight = jnp.zeros((n, tok_rows), f32)
        for k in range(routes_ref.shape[0]):
            same = routes_ref[k : k + 1, :] == number
            chosen = jnp.where(same, 1.0, chosen)
            weight = jnp.where(same, route_weight_ref[k : k + 1, :], weight)
        earlier = (
            lax.broadcasted_iota(jnp.int32, (tok_rows, tok_rows), 0)
            < lax.broadcasted_iota(jnp.int32, (tok_rows, tok_rows), 1)
        ).astype(f32)
        rank = jnp.dot(chosen, earlier, preferred_element_type=f32)
        rank = jnp.where(chosen > 0.5, rank, -1.0)
        slot = lax.broadcasted_iota(jnp.int32, (cap, tok_rows), 0).astype(f32)
        picks = []
        for j in range(n):
            taken = slot == rank[j : j + 1, :]
            picks.append(jnp.where(taken, 1.0, 0.0))
            slot_weight[j * cap : (j + 1) * cap, :] = jnp.where(taken, weight[j : j + 1, :], 0.0)
        pick = jnp.concatenate(picks, axis=0).astype(bf16)
        settle("expert", "expert_gain")
        normed = rms_scale(expert_in[...].astype(f32), expert_gain_ref[...]).astype(bf16)
        out = jnp.dot(pick, normed, preferred_element_type=f32).astype(bf16)
        rows[0:cap, :] = out[0:cap, :]
        outg[cap:, :] = out[cap:, :]

    def turned(values_in, gain):
        field = rms_scale(values_in.astype(f32), gain)
        lane = lax.broadcasted_iota(jnp.int32, field.shape, 1)
        first = jnp.bitwise_and(lane, HEAD // 2 - 1) < HEAD // 4
        partner = jnp.where(
            first,
            pltpu.roll(field, HEAD - HEAD // 4, axis=1),
            pltpu.roll(field, HEAD // 4, axis=1),
        )
        pieces = []
        all_rows = n * grid_rows
        for r in range(grid_rows):
            span = slice(r * GRID_W, (r + 1) * GRID_W)
            line = 2 * GRID_W + ep * grid_rows + r
            cosine = turn_ref[pl.ds(line, 1), :] + turn_ref[0:GRID_W, :]
            sine = turn_ref[pl.ds(line + all_rows, 1), :] + turn_ref[GRID_W : 2 * GRID_W, :]
            pieces.append(field[span] * cosine + partner[span] * sine)
        return jnp.concatenate(pieces, axis=0).astype(bf16)

    def turn_keys():
        settle("key", "key_gain", "turn")
        kv_all[0:local_rows, 0:HEAD] = turned(key[...], key_gain_ref[...])
        settle("value")

    def forward(j):
        if j:
            dispatch[j].wait_recv()
        to_chip[j].start()
        to_core[j].start()

    def pass_on(j):
        to_chip[j].wait_recv()
        relay[j].start()

    def compute(js):
        for name in ("gate", "up", "down"):
            settle(name)
        for j in js:
            to_core[j].wait_recv()
            relay[j].wait_recv()
        span = pl.ds(place(js[0], 0), 4 * len(js) * cap)
        taken = rows[span, :]
        hidden = clamped_unit(
            jnp.dot(taken, gate[...], preferred_element_type=f32),
            jnp.dot(taken, up[...], preferred_element_type=f32),
        )
        part[span, :] = jnp.dot(hidden, down[...], preferred_element_type=f32).astype(bf16)
        for j in js:
            p_core[j].start()

    def wide(ref, start, size):
        return ref[pl.ds(start, size), :].astype(f32)

    def reduce_core(j):
        p_core[j].wait_recv()
        part_sum[pl.ds(j * cap, cap), :] = (
            wide(part, place(j, 1), cap) + wide(part_in, (2 * j + 1) * cap, cap)
        ).astype(bf16)
        p_chip[j].start()

    def reduce_chip(j):
        p_chip[j].wait_recv()
        summed = (
            wide(part, place(j, 0), cap)
            + wide(part_in, 2 * j * cap, cap)
            + wide(part_xin, j * cap, cap)
        ).astype(bf16)
        if j == 0:
            ret[pl.ds(0, cap), :] = summed
        else:
            final[pl.ds(j * cap, cap), :] = summed
            give_back[j].start()

    def kv_stage(s):
        if s:
            for copy in kv_stages[s - 1]:
                copy.wait_recv()
        for copy in kv_stages[s]:
            copy.start()

    def attend(head):
        settle("query", "query_gain", "turn")
        while kv_last:
            kv_last.pop().wait_recv()
        column = slice(head * HEAD, (head + 1) * HEAD)
        scores = lax.dot_general(
            turned(query[:, column], query_gain_ref[...]),
            kv_all[:, :HEAD],
            (((1,), (1,)), ((), ())),
            preferred_element_type=f32,
        ) * (HEAD ** (-0.5))
        expo = jnp.exp(scores - jnp.max(scores, axis=-1, keepdims=True))
        total = jnp.sum(expo, axis=-1, keepdims=True)
        summed = jnp.dot(expo.astype(bf16), kv_all[:, HEAD:], preferred_element_type=f32)
        att[:, column] = (summed / total).astype(bf16)

    def block_of(bits):
        return pl.multiple_of(flip(tp, bits) * share, share)

    mix_core = [
        remote(
            at(proj, block_of(1 + 2 * i), share),
            at(proj_in, i * share, share),
            mix_send.at[i],
            mix_recv.at[i],
            0,
            1,
        )
        for i in range(2)
    ]
    mix_chip = remote(proj_sum, proj_xin, mix_send.at[2], mix_recv.at[2], 0, 2)

    def project():
        settle("out")
        proj[...] = jnp.dot(att[...], out_w[...], preferred_element_type=f32).astype(bf16)
        for copy in mix_core:
            copy.start()

    def mix_reduce():
        for copy in mix_core:
            copy.wait_recv()
        proj_sum[...] = (wide(proj, block_of(2), share) + wide(proj_in, share, share)).astype(bf16)
        mix_chip.start()

    def mix_finish():
        mix_chip.wait_recv()
        settle("mixer_gain")
        summed = (
            wide(proj, block_of(0), share)
            + wide(proj_in, 0, share)
            + proj_xin[...].astype(f32)
        )
        mixer_out_ref[...] = rms_scale(summed, mixer_gain_ref[...]).astype(bf16)

    def weighted(start, size):
        rest = slot_weight[start : start + size, :]
        total = None
        for _ in range(3):
            piece = rest.astype(bf16)
            rest = rest - piece.astype(f32)
            term = lax.dot_general(
                piece,
                ret[start : start + size, :],
                (((0,), (0,)), ((), ())),
                preferred_element_type=f32,
            )
            total = term if total is None else total + term
        return total

    def gather():
        for copy in give_back[1:]:
            copy.wait_recv()
        combined[...] = weighted(cap, (n - 1) * cap)

    def finish():
        settle("ffn_gain")
        total = combined[...] + weighted(0, cap)
        expert_out_ref[...] = rms_scale(total, ffn_gain_ref[...]).astype(bf16)

    actions = {
        "F": forward,
        "D": lambda j: dispatch[j].start(),
        "R": pass_on,
        "P": reduce_core,
        "G": reduce_chip,
        "K": kv_stage,
        "A": attend,
    }
    single = {
        "KR": turn_keys,
        "O": project,
        "M": mix_reduce,
        "N": mix_finish,
        "Q": gather,
        "E": finish,
    }
    with jax.named_scope("route"):
        route()
    with jax.named_scope("barrier"):
        pl.semaphore_wait(barrier, len(peers))
    for step in STEPS:
        with jax.named_scope(step):
            if step in single:
                single[step]()
            elif step[0] == "C":
                compute([int(c) for c in step[1:]])
            else:
                actions[step[0]](int(step[1:]))
    with jax.named_scope("drain"):
        for copy in (
            [c for stage in kv_stages for c in stage]
            + dispatch[1:]
            + to_core
            + to_chip
            + relay
            + p_core
            + p_chip
            + give_back[1:]
            + mix_core
            + [mix_chip]
        ):
            copy.wait_send()


def fused_local(
    queries,
    keys,
    values,
    query_gain,
    key_gain,
    out_weight,
    mixer_gain,
    expert_in,
    routes,
    route_weights,
    expert_gain,
    gate_w,
    up_w,
    down_w,
    ffn_out_gain,
):
    n = lax.axis_size("ep")
    local_rows, query_width = queries.shape
    tok_rows, width = expert_in.shape
    cap = capacity_of(tok_rows, routes.shape[1], n)
    hidden = gate_w.shape[2]
    share = local_rows // 4
    table = turn_table(n * local_rows // GRID_W)
    vmem = pl.BlockSpec(memory_space=pltpu.VMEM)
    anywhere = pl.BlockSpec(memory_space=pl.ANY)
    bf16, f32 = jnp.bfloat16, jnp.float32
    dma = pltpu.SemaphoreType.DMA

    return pl.pallas_call(
        fused_kernel,
        out_shape=(
            pltpu.VMEM((share, width), bf16),
            pltpu.VMEM((tok_rows, width), bf16),
        ),
        in_specs=[anywhere] * 16,
        out_specs=(vmem, vmem),
        scratch_shapes=[
            pltpu.VMEM((1, width), f32),
            pltpu.VMEM((routes.shape[1], tok_rows), jnp.int32),
            pltpu.VMEM((routes.shape[1], tok_rows), f32),
            pltpu.VMEM((1, HEAD), f32),
            pltpu.VMEM((1, HEAD), f32),
            pltpu.VMEM(table.shape, f32),
            pltpu.VMEM((1, width), f32),
            pltpu.VMEM((1, width), f32),
            pltpu.VMEM((local_rows, query_width), bf16),
            pltpu.VMEM((local_rows, HEAD), bf16),
            pltpu.VMEM((tok_rows, width), bf16),
            pltpu.VMEM((query_width, width), bf16),
            pltpu.VMEM((width, hidden), bf16),
            pltpu.VMEM((width, hidden), bf16),
            pltpu.VMEM((hidden, width), bf16),
            pltpu.VMEM((n * local_rows, 2 * HEAD), bf16),
            pltpu.VMEM((local_rows, query_width), bf16),
            pltpu.VMEM((local_rows, width), bf16),
            pltpu.VMEM((2 * share, width), bf16),
            pltpu.VMEM((share, width), bf16),
            pltpu.VMEM((share, width), bf16),
            pltpu.VMEM((n * cap, width), bf16),
            pltpu.VMEM((n * cap, tok_rows), f32),
            pltpu.VMEM((4 * n * cap, width), bf16),
            pltpu.VMEM((4 * n * cap, width), bf16),
            pltpu.VMEM((2 * n * cap, width), bf16),
            pltpu.VMEM((n * cap, width), bf16),
            pltpu.VMEM((n * cap, width), bf16),
            pltpu.VMEM((n * cap, width), bf16),
            pltpu.VMEM((n * cap, width), bf16),
            pltpu.VMEM((tok_rows, width), f32),
            dma((16,)),
        ]
        + [dma((n,))] * 16
        + [dma((3,))] * 2,
        compiler_params=pltpu.CompilerParams(
            collective_id=0, has_side_effects=True, vmem_limit_bytes=60 * 2**20
        ),
    )(
        queries,
        keys,
        values,
        expert_in,
        out_weight,
        gate_w[0],
        up_w[0],
        down_w[0],
        expert_gain[None],
        routes.T,
        route_weights.T,
        query_gain[None],
        key_gain[None],
        table,
        mixer_gain[None],
        ffn_out_gain[None],
    )


def local(
    queries,
    keys,
    values,
    query_gain,
    key_gain,
    out_weight,
    mixer_gain,
    expert_in,
    routes,
    route_weights,
    expert_gain,
    gate_w,
    up_w,
    down_w,
    ffn_out_gain,
):
    if fused_fits(queries, keys, expert_in, routes, gate_w):
        return fused_local(
            queries, keys, values, query_gain, key_gain, out_weight, mixer_gain, expert_in, routes,
            route_weights, expert_gain, gate_w, up_w, down_w, ffn_out_gain,
        )
    mixer_out = mixer_half(queries, keys, values, query_gain, key_gain, out_weight, mixer_gain)
    expert_out = expert_half(
        expert_in, routes, route_weights, expert_gain, gate_w, up_w, down_w, ffn_out_gain
    )
    return (mixer_out, expert_out)


def solution(mesh):
    in_specs = (
        P("ep", "tp"),
        P("ep", "tp"),
        P("ep", "tp"),
        P(),
        P(),
        P("tp", None),
        P(),
        P(("ep", "tp"), None),
        P(("ep", "tp"), None),
        P(("ep", "tp"), None),
        P(),
        P("ep", None, "tp"),
        P("ep", None, "tp"),
        P("ep", "tp", None),
        P(),
    )
    out_specs = (P(("ep", "tp"), None), P(("ep", "tp"), None))
    return jax.shard_map(local, mesh=mesh, in_specs=in_specs, out_specs=out_specs, check_vma=False)
```
